32 devices in a mesh: kv: 8 (over z, x), tp: 4 (over y, core).
Axes of the slice: x: 2, y: 2, z: 4, core: 2. Of those that a mesh axis runs over, the one named last changes fastest.
Arguments:
- tokens: bfloat16 [16, 4096], P(None, ('kv', 'tp')), may hold values from -24 to 24
- live_lengths: int32 [16], replicated, may hold values from 64 to 4096, as said below
- kv_cache: bfloat16 [16, 4096, 2048], P(None, 'kv', 'tp'), may hold values from -128 to 128
- gate_sums: float32 [16, 16, 4096], P(None, 'tp', 'kv'), may hold values from -4096 to 0, as said below
- w_query: bfloat16 [4096, 4096], P('kv', 'tp'), may hold values from -0.09375 to 0.09375
- w_key: bfloat16 [4096, 1024], P('kv', 'tp'), may hold values from -0.09375 to 0.09375
- w_value: bfloat16 [4096, 1024], P('kv', 'tp'), may hold values from -0.09375 to 0.09375
- w_forget: bfloat16 [4096, 16], replicated, may hold values from -0.09375 to 0.09375
- forget_bias: float32 [16], replicated, may hold values from -1 to 2
- w_out: bfloat16 [4096, 4096], P('tp', 'kv'), may hold values from -0.5 to 0.5
- first_gain: float32 [4096], P(('kv', 'tp')), may hold values from 0 to 4
- w_gate: bfloat16 [4096, 11264], P('kv', 'tp'), may hold values from -0.09375 to 0.09375
- w_up: bfloat16 [4096, 11264], P('kv', 'tp'), may hold values from -0.09375 to 0.09375
- w_down: bfloat16 [11264, 4096], P('tp', 'kv'), may hold values from -0.078125 to 0.078125
- second_gain: float32 [4096], P(('kv', 'tp')), may hold values from 0 to 4
Outputs:
- layer_out: bfloat16 [16, 4096], P(None, ('kv', 'tp'))
The draws below stay inside these ranges and needn't reach their ends.
Inputs may be any that keep to these rules, and one draw needn't show every extreme that they name: `live_lengths`: at least one sequence has length exactly 4096. `gate_sums`: entries at positions at or beyond the sequence's length are 0.
All inputs are finite; a program needn't handle non-finite values.
Results may differ from the reference program's by a relative error of at most 0.019.
Values may be sent and summed in bfloat16 or wider, within the bound.
A program may use at most 64 MiB of HBM per device.

```python
import jax
import jax.numpy as jnp
from jax import lax

D = 4096
DH = 64
KEY_HEAD_COUNT = 16
GROUP = 4
H = 64
FF = 11264
SEQUENCE_COUNT = 16
P_DEV = 512
LEN = 4096


def sequence_lengths(key):
    base_key = jax.random.fold_in(key, 701)
    short_key, long_key, order_key = jax.random.split(base_key, 3)
    short_floor = max(LEN // 64, 2)
    short_lengths = jax.random.randint(short_key, (SEQUENCE_COUNT,), short_floor, max(LEN // 8, short_floor) + 1)
    long_lengths = jax.random.randint(long_key, (SEQUENCE_COUNT,), max(LEN // 2, 2), LEN + 1)
    ranking = jax.random.permutation(order_key, SEQUENCE_COUNT)
    chosen = jnp.where(ranking < max(SEQUENCE_COUNT // 4, 1), long_lengths, short_lengths)
    return jnp.where(ranking == 0, LEN, chosen).astype(jnp.int32)


def column_scales(key, rise_factor):
    jitter_strength = jax.random.uniform(key, (D,), jnp.float32, 0.8, 1.25)
    where_col = jnp.arange(D, dtype=jnp.float32) / max(D - 1, 1)
    return jitter_strength * jnp.exp(jnp.log(rise_factor) * (where_col - 0.5))


def token_rows(key):
    base_key = jax.random.fold_in(key, 702)
    noise_key, scale_key = jax.random.split(base_key, 2)
    noise_draw = jnp.clip(jax.random.normal(noise_key, (SEQUENCE_COUNT, D), jnp.float32), -6.0, 6.0)
    scales = column_scales(scale_key, 3.0)[None, :]
    return noise_draw * scales + scales


def query_weight(key):
    base_key = jax.random.fold_in(key, 703)
    return jnp.clip(jax.random.normal(base_key, (D, H * DH), jnp.float32), -6.0, 6.0) * D ** (-0.5)


def log_uniform(key, array_shape, lower_end, upper_end):
    return jnp.exp(jax.random.uniform(key, array_shape, jnp.float32, jnp.log(lower_end), jnp.log(upper_end)))


def rising_gain(key, salt_value):
    base_key = jax.random.fold_in(key, salt_value)
    return column_scales(base_key, 3.0)


def draw_tokens(key, part):
    return token_rows(key).astype(jnp.bfloat16)


def draw_live_lengths(key, part):
    return sequence_lengths(key)


def draw_w_query(key, part):
    return query_weight(key).astype(jnp.bfloat16)


def draw_first_gain(key, part):
    return rising_gain(key, 706)


def draw_second_gain(key, part):
    return rising_gain(key, 707)


def draw_kv_cache(key, part):
    base_key = jax.random.fold_in(key, 704)
    noise_key, offset_key = jax.random.split(base_key, 2)
    entries = jnp.clip(jax.random.normal(noise_key, (SEQUENCE_COUNT, LEN, KEY_HEAD_COUNT, 2, DH), jnp.float32), -6.0, 6.0)
    block_count = (LEN + 63) // 64
    offsets = jnp.clip(jax.random.normal(offset_key, (SEQUENCE_COUNT, block_count, 1, KEY_HEAD_COUNT, 1, DH), jnp.float32), -3.0, 3.0)
    offsets = jnp.broadcast_to(offsets, (SEQUENCE_COUNT, block_count, 64, KEY_HEAD_COUNT, 1, DH)).reshape(SEQUENCE_COUNT, block_count * 64, KEY_HEAD_COUNT, 1, DH)[:, :LEN]
    slot_pick = jnp.array([0.0, 1.0], jnp.float32).reshape(1, 1, 1, 2, 1)
    entries = entries + offsets * slot_pick
    return entries.reshape(SEQUENCE_COUNT, LEN, KEY_HEAD_COUNT * 2 * DH).astype(jnp.bfloat16)


def draw_gate_sums(key, part):
    base_key = jax.random.fold_in(key, 705)
    head_key, fast_key, slow_key, block_key, rough_key, location_random_key, depth_key = jax.random.split(base_key, 7)
    length_values = sequence_lengths(key)
    head_order = jax.random.permutation(head_key, KEY_HEAD_COUNT)
    quick_decay_heads = head_order < max(KEY_HEAD_COUNT // 2, 1)
    fast_rate = log_uniform(fast_key, (SEQUENCE_COUNT, KEY_HEAD_COUNT, 1), 0.04, 0.12)
    slow_rate = log_uniform(slow_key, (SEQUENCE_COUNT, KEY_HEAD_COUNT, 1), 0.2, 0.8) / LEN
    increment_ratio = jnp.where(quick_decay_heads[None, :, None], fast_rate, slow_rate)
    block_count = (LEN + P_DEV - 1) // P_DEV
    block_multiplier = log_uniform(block_key, (SEQUENCE_COUNT, KEY_HEAD_COUNT, block_count, 1), 0.5, 2.0)
    block_multiplier = jnp.broadcast_to(block_multiplier, (SEQUENCE_COUNT, KEY_HEAD_COUNT, block_count, P_DEV)).reshape(SEQUENCE_COUNT, KEY_HEAD_COUNT, block_count * P_DEV)[:, :, :LEN]
    jitter_strength = jax.random.uniform(rough_key, (SEQUENCE_COUNT, KEY_HEAD_COUNT, LEN), jnp.float32, 0.5, 1.5)
    spike_locations = jax.random.randint(location_random_key, (SEQUENCE_COUNT, KEY_HEAD_COUNT, 3), 0, length_values[:, None, None])
    depth_values = jnp.log(jax.random.uniform(depth_key, (SEQUENCE_COUNT, KEY_HEAD_COUNT, 3), jnp.float32, 0.5, 0.8))
    position_selector = jnp.arange(LEN, dtype=jnp.int32)
    spike_decrease = jnp.sum(jnp.where(position_selector[None, None, None, :] == spike_locations[..., None], depth_values[..., None], 0.0), axis=2)
    spike_decrease = jnp.where(quick_decay_heads[None, :, None], 0.0, spike_decrease)
    logarithm_gate_values = -increment_ratio * block_multiplier * jitter_strength + spike_decrease
    live_mask = position_selector[None, None, :] < length_values[:, None, None]
    masked = jnp.where(live_mask, logarithm_gate_values, 0.0)
    suffix_sum = jnp.flip(jnp.cumsum(jnp.flip(masked, axis=-1), axis=-1), axis=-1) - masked
    return suffix_sum


def spiked(drawn, own_key, source, target, blocks, factor):
    owner, partner = [(jnp.arange(drawn.shape[axis_at]) // (drawn.shape[axis_at] // blocks)).reshape([-1 if axis == axis_at else 1 for axis in range(drawn.ndim)]) for axis_at in (source, target)]
    chosen = jax.random.permutation(own_key, blocks)[partner]
    strong = (owner == chosen) | (owner == (partner + blocks // 2) % blocks)
    return jnp.where(strong, factor * drawn, drawn)


def block_scale(own_key, extent, shards, least, largest):
    def one(dim, parts):
        steps = jax.random.uniform(jax.random.fold_in(jax.random.fold_in(own_key, 6), dim), (parts,), jnp.float32, least / len(shards), largest / len(shards))
        return jnp.repeat(jnp.exp(steps), extent[dim] // parts).reshape((-1,) + (1,) * (len(extent) - dim - 1))

    loudness = one(*shards[0])
    for cut in shards[1:]:
        loudness = loudness * one(*cut)
    return loudness


def scatter_about(rng, extent, width, bound, cuts=(), kind=jnp.bfloat16):
    level = block_scale(rng, extent, cuts, -0.22, 0.18) if cuts else 1.0
    values = jax.random.normal(rng, extent, jnp.float32) * width * level
    return jnp.minimum(jnp.maximum(values, -bound), bound).astype(kind)


def gaussian_with(own_key, extent, deviation, most, cuts, heavy, kind=jnp.bfloat16):
    drawn = deviation * jax.random.normal(own_key, extent, jnp.float32)
    if cuts:
        drawn = drawn * block_scale(own_key, extent, cuts, -0.22, 0.18)
    return jnp.clip(spiked(drawn, jax.random.fold_in(own_key, 3), *heavy), -most, most).astype(kind)


def setup_inputs(seed: int = 0) -> dict:
    arg_keys = jax.random.split(jax.random.key(seed), 16)
    tokens = draw_tokens(jax.random.fold_in(arg_keys[15], 71), 0)
    live_lengths = draw_live_lengths(jax.random.fold_in(arg_keys[15], 71), 0)
    kv_cache = draw_kv_cache(jax.random.fold_in(arg_keys[15], 71), 0)
    gate_sums = draw_gate_sums(jax.random.fold_in(arg_keys[15], 71), 0)
    w_query = draw_w_query(jax.random.fold_in(arg_keys[15], 71), 0)
    w_key = scatter_about(arg_keys[5], (D, KEY_HEAD_COUNT * DH), D ** -0.5, 0.09375, ((0, 8), (1, 4)))
    w_value = scatter_about(arg_keys[6], (D, KEY_HEAD_COUNT * DH), D ** -0.5, 0.09375, ((0, 8), (1, 4)))
    w_forget = scatter_about(arg_keys[7], (D, KEY_HEAD_COUNT), D ** -0.5, 0.09375)
    forget_bias = jnp.clip(jax.random.uniform(arg_keys[8], (KEY_HEAD_COUNT,), jnp.float32, -1.0, 2.0), -1.0, 2.0)
    w_out = gaussian_with(arg_keys[9], (H * DH, D), (H * DH // 16) ** -0.5, 0.5, ((0, 4), (1, 8)), (0, 1, 8, 2.0))
    first_gain = draw_first_gain(jax.random.fold_in(arg_keys[15], 71), 0)
    w_gate = scatter_about(arg_keys[11], (D, FF), D ** -0.5, 0.09375, ((0, 8), (1, 4)))
    w_up = scatter_about(arg_keys[12], (D, FF), D ** -0.5, 0.09375, ((0, 8), (1, 4)))
    w_down = gaussian_with(arg_keys[13], (FF, D), FF ** -0.5, 0.078125, ((0, 4), (1, 8)), (0, 1, 8, 2.0))
    second_gain = draw_second_gain(jax.random.fold_in(arg_keys[15], 71), 0)
    return {"tokens": tokens, "live_lengths": live_lengths, "kv_cache": kv_cache, "gate_sums": gate_sums, "w_query": w_query, "w_key": w_key, "w_value": w_value, "w_forget": w_forget, "forget_bias": forget_bias, "w_out": w_out, "first_gain": first_gain, "w_gate": w_gate, "w_up": w_up, "w_down": w_down, "second_gain": second_gain}


EPSILON = 1e-05

def layer_norm(mixture, norm_gain):
    centre = lax.optimization_barrier(jnp.mean(mixture, axis=-1, keepdims=True))
    spread = lax.optimization_barrier(jnp.mean(jnp.square(mixture - centre), axis=-1, keepdims=True))
    return ((mixture - centre) * lax.rsqrt(spread + EPSILON) * norm_gain).astype(jnp.bfloat16)

def attend_sequence(pieces):
    query_row, new_key, new_value, new_gate, cache_rows, gate_row, length = pieces
    queries = query_row.astype(jnp.float32).reshape(KEY_HEAD_COUNT, GROUP, DH)
    blocks = cache_rows.astype(jnp.float32).reshape(LEN, KEY_HEAD_COUNT, 2, DH)
    score_scale = DH ** (-0.5)
    scores = jnp.einsum('gjd,sgd->gjs', queries, blocks[:, :, 0, :]) * score_scale
    scores = scores + gate_row[:, None, :] + new_gate[:, None, None]
    live_mask = jnp.arange(LEN, dtype=jnp.int32) < length
    own_score = jnp.einsum('gjd,gd->gj', queries, new_key.astype(jnp.float32).reshape(KEY_HEAD_COUNT, DH)) * score_scale
    row_top = jnp.maximum(lax.optimization_barrier(jnp.max(jnp.where(live_mask, scores, -jnp.inf), axis=-1)), own_score)
    weights = jnp.where(live_mask, jnp.exp(scores - row_top[..., None]), 0.0)
    own_weight = jnp.exp(own_score - row_top)
    weight_total = lax.optimization_barrier(jnp.sum(weights, axis=-1)) + own_weight
    rounded = lax.optimization_barrier(weights.astype(jnp.bfloat16)).astype(jnp.float32)
    own_rounded = lax.optimization_barrier(own_weight.astype(jnp.bfloat16)).astype(jnp.float32)
    summed = jnp.einsum('gjs,sgd->gjd', rounded, blocks[:, :, 1, :])
    summed = summed + own_rounded[..., None] * new_value.astype(jnp.float32).reshape(KEY_HEAD_COUNT, 1, DH)
    return (summed / weight_total[..., None]).reshape(KEY_HEAD_COUNT * GROUP * DH).astype(jnp.bfloat16)

def reference(tokens, live_lengths, kv_cache, gate_sums, w_query, w_key, w_value, w_forget, forget_bias, w_out, first_gain, w_gate, w_up, w_down, second_gain):
    queries = jnp.dot(tokens, w_query, preferred_element_type=jnp.float32).astype(jnp.bfloat16)
    new_keys = jnp.dot(tokens, w_key, preferred_element_type=jnp.float32).astype(jnp.bfloat16)
    new_values = jnp.dot(tokens, w_value, preferred_element_type=jnp.float32).astype(jnp.bfloat16)
    new_gates = jax.nn.log_sigmoid(jnp.dot(tokens, w_forget, preferred_element_type=jnp.float32) + forget_bias)
    attended = lax.map(attend_sequence, (queries, new_keys, new_values, new_gates, kv_cache, gate_sums, live_lengths))
    attn_out = jnp.dot(attended, w_out, preferred_element_type=jnp.float32)
    after_mix = layer_norm(tokens.astype(jnp.float32) + attn_out, first_gain)
    gate_units = jnp.dot(after_mix, w_gate, preferred_element_type=jnp.float32)
    up_units = jnp.dot(after_mix, w_up, preferred_element_type=jnp.float32)
    hidden = (jax.nn.silu(gate_units) * up_units).astype(jnp.bfloat16)
    ffn_out = jnp.dot(hidden, w_down, preferred_element_type=jnp.float32)
    return layer_norm(after_mix.astype(jnp.float32) + ffn_out, second_gain)
```

```python
import functools

import jax
import jax.numpy as jnp
from jax import lax
from jax.experimental import pallas as pl
from jax.experimental.pallas import tpu as pltpu
from jax.sharding import PartitionSpec as P

D = 4096
DH = 64
GROUP = 4


EPSILON = 1e-05
EMPTY_SCORE = -1e30


def combined_all(shard, axis, combine):
    everything = jax.tree.map(lambda part: lax.all_gather(part, axis), shard)
    initial = jax.tree.map(lambda part: part[0], everything)

    def lap(k, so_far):
        return combine(so_far, jax.tree.map(lambda part: part[k], everything))

    return lax.fori_loop(1, lax.axis_size(axis), lap, initial)


def combine_parts(earlier, later):
    earlier_top, earlier_total, earlier_sum = earlier
    later_top, later_total, later_sum = later
    joint_top = jnp.maximum(earlier_top, later_top)
    earlier_scale = jnp.exp(earlier_top - joint_top)
    later_scale = jnp.exp(later_top - joint_top)
    joint_total = earlier_total * earlier_scale + later_total * later_scale
    joint_sum = earlier_sum * earlier_scale[..., None] + later_sum * later_scale[..., None]
    return (joint_top, joint_total, joint_sum)


def normalize_block(mixture, norm_gain):
    row_sum, row_square = lax.psum(
        (jnp.sum(mixture, axis=1), jnp.sum(mixture * mixture, axis=1)), "kv"
    )
    centre = row_sum / D
    spread = row_square / D - centre * centre
    scaled = (mixture - centre[:, None]) * lax.rsqrt(spread[:, None] + EPSILON) * norm_gain
    return scaled.astype(jnp.bfloat16)


def on_device(
    tokens,
    live_lengths,
    kv_cache,
    gate_sums,
    w_query,
    w_key,
    w_value,
    w_forget,
    forget_bias,
    w_out,
    first_gain,
    w_gate,
    w_up,
    w_down,
    second_gain,
):
    sequences = tokens.shape[0]
    own_cols = tokens.shape[1]
    gains_pair = jnp.stack([first_gain, second_gain], axis=0)
    wide_rows, wide_gains = (
        lax.all_gather(tokens.astype(jnp.float32), "tp", axis=1, tiled=True),
        lax.all_gather(gains_pair, "tp", axis=1, tiled=True),
    )
    block_rows = wide_rows.astype(jnp.bfloat16)
    row_count = block_rows.shape[1]
    row_start = lax.axis_index("kv") * row_count
    local_heads = kv_cache.shape[2] // (2 * DH)
    head_start = lax.axis_index("tp") * local_heads
    forget_rows = lax.dynamic_slice(w_forget, (row_start, head_start), (row_count, local_heads))
    query_part = jnp.dot(block_rows, w_query, preferred_element_type=jnp.float32)
    key_part = jnp.dot(block_rows, w_key, preferred_element_type=jnp.float32)
    value_part = jnp.dot(block_rows, w_value, preferred_element_type=jnp.float32)
    forget_part = jnp.dot(block_rows, forget_rows, preferred_element_type=jnp.float32)
    query_sum, key_sum, value_sum, forget_sum = lax.psum(
        (query_part, key_part, value_part, forget_part), "kv"
    )
    queries = query_sum.astype(jnp.bfloat16).reshape(sequences, local_heads, GROUP, DH)
    new_keys = key_sum.astype(jnp.bfloat16).reshape(sequences, local_heads, DH)
    new_values = value_sum.astype(jnp.bfloat16).reshape(sequences, local_heads, DH)
    bias_rows = lax.dynamic_slice_in_dim(forget_bias, head_start, local_heads)
    new_gate = jax.nn.log_sigmoid(forget_sum + bias_rows)
    positions = kv_cache.shape[1]
    cached = kv_cache.reshape(sequences, positions, local_heads, 2, DH)
    score_scale = DH ** (-0.5)
    scores = (
        jnp.einsum(
            "bgjd,bpgd->bgjp", queries, cached[:, :, :, 0], preferred_element_type=jnp.float32
        )
        * score_scale
    )
    scores = scores + gate_sums[:, :, None, :] + new_gate[:, :, None, None]
    position_selector = lax.axis_index("kv") * positions + jnp.arange(positions, dtype=jnp.int32)
    live_mask = (position_selector[None, :] < live_lengths[:, None])[:, None, None, :]
    local_top = jnp.max(jnp.where(live_mask, scores, EMPTY_SCORE), axis=-1)
    weights = jnp.where(live_mask, jnp.exp(scores - local_top[..., None]), 0.0)
    local_total = jnp.sum(weights, axis=-1)
    local_sum = jnp.einsum(
        "bgjp,bpgd->bgjd",
        weights.astype(jnp.bfloat16),
        cached[:, :, :, 1],
        preferred_element_type=jnp.float32,
    )
    row_top, weight_total, summed = combined_all(
        (local_top, local_total, local_sum), "kv", combine_parts
    )
    own_score = (
        jnp.einsum("bgjd,bgd->bgj", queries, new_keys, preferred_element_type=jnp.float32)
        * score_scale
    )
    final_top = jnp.maximum(row_top, own_score)
    carry_scale = jnp.exp(row_top - final_top)
    own_weight = jnp.exp(own_score - final_top)
    own_rounded = lax.optimization_barrier(own_weight.astype(jnp.bfloat16)).astype(jnp.float32)
    numerator = summed * carry_scale[..., None] + own_rounded[..., None] * new_values[
        :, :, None, :
    ].astype(jnp.float32)
    attended = (numerator / (weight_total * carry_scale + own_weight)[..., None]).astype(
        jnp.bfloat16
    )
    attended = attended.reshape(sequences, local_heads * GROUP * DH)
    attn_part = jnp.dot(attended, w_out, preferred_element_type=jnp.float32)
    attn_block = lax.psum(attn_part, "tp")
    mid_rows = normalize_block(wide_rows + attn_block, wide_gains[0])
    gate_part = jnp.dot(mid_rows, w_gate, preferred_element_type=jnp.float32)
    up_part = jnp.dot(mid_rows, w_up, preferred_element_type=jnp.float32)
    gate_full, up_full = (
        lax.psum(gate_part.astype(jnp.bfloat16), "kv").astype(jnp.float32),
        lax.psum(up_part.astype(jnp.bfloat16), "kv").astype(jnp.float32),
    )
    hidden = (jax.nn.silu(gate_full) * up_full).astype(jnp.bfloat16)
    ffn_part = jnp.dot(hidden, w_down, preferred_element_type=jnp.float32)
    ffn_block = lax.psum(ffn_part, "tp")
    out_block = normalize_block(mid_rows.astype(jnp.float32) + ffn_block, wide_gains[1])
    return lax.dynamic_slice_in_dim(out_block, lax.axis_index("tp") * own_cols, own_cols, 1)


MESH = pl.DeviceIdType.MESH
F32 = jnp.float32
BF16 = jnp.bfloat16
LANES = 128


def push(axis, peer, me, source, landing, sends, recvs):
    return pltpu.make_async_remote_copy(
        src_ref=source,
        dst_ref=landing.at[me],
        send_sem=sends.at[peer],
        recv_sem=recvs.at[me],
        device_id={axis: peer},
        device_id_type=MESH,
    )


def arrival(axis, peer, source, landing, sends, recvs):
    return pltpu.make_async_remote_copy(
        src_ref=source,
        dst_ref=landing.at[peer],
        send_sem=sends.at[peer],
        recv_sem=recvs.at[peer],
        device_id={axis: peer},
        device_id_type=MESH,
    )


def head_rows(block, odd, lane):
    moved = pltpu.roll(block, DH, 1) if odd else block
    return jnp.where(lane < DH, moved, 0.0)


def fused_kernel(
    dims,
    tokens,
    lengths,
    cache_hbm,
    gates_hbm,
    wq_hbm,
    wk_hbm,
    wv_hbm,
    wf_hbm,
    bias,
    wo_hbm,
    gain_one,
    wg_hbm,
    wu_hbm,
    wd_hbm,
    gain_two,
    out,
    wqkv,
    wf,
    cache,
    gates,
    wo,
    wg,
    wu,
    wd,
    tok_own,
    tok_all,
    qkv_part,
    qkv_in,
    qkv_own,
    qkv_all,
    q_rows,
    kv_rows,
    gate_now,
    att_part,
    att_in,
    att_own,
    att_all,
    x_own,
    x_in,
    y_own,
    y_in,
    s1_own,
    s1_in,
    s2_own,
    s2_in,
    gu_part,
    gu_in,
    hid_own,
    hid_all,
    wide,
    sems,
    tp_send,
    tp_recv,
    kv_send,
    kv_recv,
):
    seqs, k_size, t_size, heads, chunk, n_chunks, f_chunk, positions = dims
    kv = lax.axis_index("kv")
    tp = lax.axis_index("tp")
    rows_n = wq_hbm.shape[0]
    q_cols = wq_hbm.shape[1]
    kk = wk_hbm.shape[1]
    ff = wg_hbm.shape[1]
    width = wo_hbm.shape[1]
    per = seqs // k_size
    rows = heads * GROUP
    local = [
        pltpu.make_async_copy(wq_hbm, wqkv.at[:, :q_cols], sems.at[0]),
        pltpu.make_async_copy(wk_hbm, wqkv.at[:, q_cols : q_cols + kk], sems.at[1]),
        pltpu.make_async_copy(wv_hbm, wqkv.at[:, q_cols + kk :], sems.at[2]),
        pltpu.make_async_copy(
            wf_hbm.at[pl.ds(pl.multiple_of(kv * rows_n, rows_n), rows_n), :], wf, sems.at[3]
        ),
        pltpu.make_async_copy(cache_hbm, cache, sems.at[4]),
        pltpu.make_async_copy(gates_hbm, gates, sems.at[5]),
        pltpu.make_async_copy(wo_hbm, wo, sems.at[6]),
        pltpu.make_async_copy(wg_hbm, wg.at[:, :ff], sems.at[7]),
        pltpu.make_async_copy(wu_hbm, wu.at[:, :ff], sems.at[8]),
        pltpu.make_async_copy(wd_hbm, wd.at[:ff, :], sems.at[9]),
    ]
    for copy in local:
        copy.start()
    barrier = pltpu.get_barrier_semaphore()
    for i in range(1, k_size):
        pl.semaphore_signal(
            barrier, inc=1, device_id={"kv": lax.rem(kv + i, k_size)}, device_id_type=MESH
        )
    for i in range(1, t_size):
        pl.semaphore_signal(
            barrier, inc=1, device_id={"tp": lax.rem(tp + i, t_size)}, device_id_type=MESH
        )
    padded = wg.shape[1]
    if padded > ff:
        wg[:, ff:] = jnp.zeros((rows_n, padded - ff), BF16)
        wu[:, ff:] = jnp.zeros((rows_n, padded - ff), BF16)
        wd[ff:, :] = jnp.zeros((padded - ff, width), BF16)
    tok_own[:seqs, :] = tokens[...].astype(F32)
    tok_own[seqs:, :] = jnp.broadcast_to(gain_one[...], (8, LANES))
    pl.semaphore_wait(barrier, k_size - 1 + t_size - 1)

    def tp_all(phase, own, landing):
        s, r = tp_send.at[phase], tp_recv.at[phase]
        for i in range(1, t_size):
            push("tp", lax.rem(tp + i, t_size), tp, own, landing, s, r).start()
        landing[tp] = own[...]
        for i in range(1, t_size):
            arrival("tp", lax.rem(tp + i, t_size), own, landing, s, r).wait_recv()

    def kv_all(phase, own, landing):
        s, r = kv_send.at[phase], kv_recv.at[phase]

        def go(i, c):
            push("kv", lax.rem(kv + i, k_size), kv, own, landing, s, r).start()
            return c

        def come(i, c):
            arrival("kv", lax.rem(kv + i, k_size), own, landing, s, r).wait_recv()
            return c

        lax.fori_loop(1, k_size, go, 0)
        landing[kv] = own[...]
        lax.fori_loop(1, k_size, come, 0)

    tp_all(0, tok_own, tok_all)
    wide_rows = jnp.concatenate([tok_all[t, :seqs, :] for t in range(t_size)], axis=1)
    wide_gain = jnp.concatenate([tok_all[t, seqs : seqs + 1, :] for t in range(t_size)], axis=1)
    wide[...] = wide_rows
    block = wide_rows.astype(BF16)
    for n in range(4):
        local[n].wait()
    for c in range(n_chunks - 1):
        qkv_part[c] = jnp.dot(
            block, wqkv[:, c * chunk : (c + 1) * chunk], preferred_element_type=F32
        )
    kv_heads = wf.shape[1]
    qkv_part[n_chunks - 1] = jnp.zeros((seqs, chunk), F32)
    qkv_part[n_chunks - 1, :, :kv_heads] = jnp.dot(block, wf[...], preferred_element_type=F32)
    s, r = kv_send.at[0], kv_recv.at[0]
    s2, r2 = kv_send.at[1], kv_recv.at[1]

    def qkv_go(i, c):
        peer = lax.rem(kv + i, k_size)

        @pl.when(peer < n_chunks)
        def _():
            push("kv", peer, kv, qkv_part.at[peer], qkv_in, s, r).start()

        return c

    lax.fori_loop(1, k_size, qkv_go, 0)

    @pl.when(kv < n_chunks)
    def _():
        qkv_in[kv] = qkv_part[kv]

        def come(i, c):
            peer = lax.rem(kv + i, k_size)
            arrival("kv", peer, qkv_part.at[0], qkv_in, s, r).wait_recv()
            return c

        lax.fori_loop(1, k_size, come, 0)
        total = qkv_in[0]
        for k in range(1, k_size):
            total = total + qkv_in[k]
        scale = jnp.where(kv < q_cols // chunk, DH**-0.5, 1.0).astype(F32)
        rounded = total.astype(BF16).astype(F32) * scale
        exact = jnp.full((seqs, chunk), kv, jnp.int32) == n_chunks - 1
        qkv_own[...] = jnp.where(exact, total, rounded)

        def go(i, c):
            push("kv", lax.rem(kv + i, k_size), kv, qkv_own, qkv_all, s2, r2).start()
            return c

        lax.fori_loop(1, k_size, go, 0)
        qkv_all[kv] = qkv_own[...]

    def qkv_come(i, c):
        peer = lax.rem(kv + i, k_size)

        @pl.when(peer < n_chunks)
        def _():
            arrival("kv", peer, qkv_own, qkv_all, s2, r2).wait_recv()

        return c

    lax.fori_loop(1, k_size, qkv_come, 0)
    lane = lax.broadcasted_iota(jnp.int32, (seqs, LANES), 1)

    def unit(start):
        return qkv_all[start // chunk, :, start % chunk : start % chunk + LANES]

    for h in range(rows):
        start = h * DH
        base = start // LANES * LANES
        q_rows[pl.ds(h, seqs, stride=rows), :] = head_rows(unit(base), start % LANES != 0, lane)
    for g in range(heads):
        base = g * DH // LANES * LANES
        odd = g % 2 == 1
        keys = unit(q_cols + base)
        values = unit(q_cols + kk + base)
        keys = pltpu.roll(keys, DH, 1) if odd else keys
        values = values if odd else pltpu.roll(values, DH, 1)
        pair = jnp.where(lane < DH, keys, values)
        for j in range(GROUP):
            kv_rows[pl.ds(g * GROUP + j, seqs, stride=rows), :] = pair
    logits = qkv_all[n_chunks - 1, :, :kv_heads] + bias[...]
    gate_now[:, :kv_heads] = jnp.minimum(logits, 0.0) - jnp.log(1.0 + jnp.exp(-jnp.abs(logits)))
    local[4].wait()
    local[5].wait()
    row_p = lax.broadcasted_iota(jnp.int32, (rows, positions), 0) // GROUP
    pos = lax.broadcasted_iota(jnp.int32, (rows, positions), 1) + kv * positions
    row_l = lax.broadcasted_iota(jnp.int32, (rows, LANES), 0) // GROUP
    lane_l = lax.broadcasted_iota(jnp.int32, (rows, LANES), 1)
    row_g = lax.broadcasted_iota(jnp.int32, (rows, kv_heads), 0) // GROUP
    lane_g = lax.broadcasted_iota(jnp.int32, (rows, kv_heads), 1)

    def attend(b):
        q = q_rows[pl.ds(pl.multiple_of(b * rows, rows), rows), :]
        spread = jnp.concatenate(
            [jnp.where(row_l == g, q, 0.0).astype(BF16) for g in range(heads)], axis=1
        )
        slab = cache[b]
        scores = lax.dot_general(
            spread, slab, (((1,), (1,)), ((), ())), preferred_element_type=F32
        )
        gate_rows = gates[b]
        gate = jnp.broadcast_to(gate_rows[0:1], (rows, positions))
        for g in range(1, heads):
            gate = jnp.where(row_p == g, gate_rows[g : g + 1], gate)
        fresh = jnp.sum(
            jnp.where(lane_g == row_g + tp * heads, gate_now[pl.ds(b, 1), :kv_heads], 0.0),
            axis=1,
            keepdims=True,
        )
        scores = scores + gate + fresh
        live = pos < lengths[b]
        scores = jnp.where(live, scores, EMPTY_SCORE)
        top = jnp.max(scores, axis=1, keepdims=True)
        weights = jnp.where(live, jnp.exp(scores - top), 0.0)
        total = jnp.sum(weights, axis=1, keepdims=True)
        mixed = jnp.dot(weights.astype(BF16), slab, preferred_element_type=F32)
        own = mixed[:, :LANES]
        for g in range(1, heads):
            own = jnp.where(row_l == g, mixed[:, g * LANES : (g + 1) * LANES], own)
        own = jnp.where(lane_l < DH // 2, top, jnp.where(lane_l < DH, total, own))
        return own

    sa, ra = kv_send.at[2], kv_recv.at[2]

    def att_go(i, c):
        peer = lax.rem(kv + i, k_size)
        for e in range(per):
            att_part[peer, e] = attend(peer * per + e)

        @pl.when(i < k_size)
        def _():
            push("kv", peer, kv, att_part.at[peer], att_in, sa, ra).start()

        return c

    lax.fori_loop(1, k_size + 1, att_go, 0)
    att_in[kv] = att_part[kv]

    def att_come(i, c):
        arrival("kv", lax.rem(kv + i, k_size), att_part.at[0], att_in, sa, ra).wait_recv()
        return c

    lax.fori_loop(1, k_size, att_come, 0)
    for e in range(per):
        at = pl.ds(pl.multiple_of((kv * per + e) * rows, rows), rows)
        q, pair = q_rows[at, :], kv_rows[at, :]
        own_score = jnp.sum(jnp.where(lane_l < DH, q * pair, 0.0), axis=1, keepdims=True)
        parts = [att_in[k, e] for k in range(k_size)]
        tops = [part[:, 0:1] for part in parts]
        high = own_score
        for top in tops:
            high = jnp.maximum(high, top)
        own_weight = jnp.exp(own_score - high)
        numer = own_weight.astype(BF16).astype(F32) * pair
        denom = own_weight
        for top, part in zip(tops, parts):
            scale = jnp.exp(top - high)
            numer = numer + part * scale
            denom = denom + part[:, DH // 2 : DH // 2 + 1] * scale
        att_own[pl.ds(e * rows, rows), :] = jnp.where(lane_l < DH, 0.0, numer / denom)
    kv_all(3, att_own, att_all)
    for k in range(k_size):
        q_rows[k * per * rows : (k + 1) * per * rows, :] = att_all[k]
    pieces = []
    for h in range(0, rows, 2):
        even = pltpu.roll(q_rows[pl.ds(h, seqs, stride=rows), :], DH, 1)
        odd = q_rows[pl.ds(h + 1, seqs, stride=rows), :]
        pieces.append(jnp.where(lane < DH, even, odd).astype(BF16))
    attended = jnp.concatenate(pieces, axis=1)
    local[6].wait()
    x_own[...] = jnp.dot(attended, wo[...], preferred_element_type=F32)

    def normed(z, phase, stat_own, stat_in):
        row_sum = jnp.sum(z, axis=1, keepdims=True)
        row_square = jnp.sum(z * z, axis=1, keepdims=True)
        stat_own[...] = jnp.where(lane == 0, row_sum, row_square)
        kv_all(phase, stat_own, stat_in)
        stats = stat_in[0]
        for k in range(1, k_size):
            stats = stats + stat_in[k]
        count = k_size * width
        centre = stats[:, 0:1] / count
        spread = stats[:, 1:2] / count - centre * centre
        return (z - centre) * lax.rsqrt(spread + EPSILON)

    tp_all(1, x_own, x_in)
    z = wide[...]
    for t in range(t_size):
        z = z + x_in[t]
    mid = (normed(z, 4, s1_own, s1_in) * wide_gain).astype(BF16)
    local[7].wait()
    local[8].wait()
    sg, rg = kv_send.at[5], kv_recv.at[5]

    def gu_go(i, c):
        peer = lax.rem(kv + i, k_size)
        at = pl.ds(pl.multiple_of(peer * f_chunk, LANES), f_chunk)
        gu_part[peer, 0] = jnp.dot(mid, wg[:, at], preferred_element_type=F32).astype(BF16)
        gu_part[peer, 1] = jnp.dot(mid, wu[:, at], preferred_element_type=F32).astype(BF16)

        @pl.when(i < k_size)
        def _():
            push("kv", peer, kv, gu_part.at[peer], gu_in, sg, rg).start()

        return c

    lax.fori_loop(1, k_size + 1, gu_go, 0)
    gu_in[kv] = gu_part[kv]

    def gu_come(i, c):
        arrival("kv", lax.rem(kv + i, k_size), gu_part.at[0], gu_in, sg, rg).wait_recv()
        return c

    lax.fori_loop(1, k_size, gu_come, 0)
    gate = gu_in[0, 0].astype(F32)
    up = gu_in[0, 1].astype(F32)
    for k in range(1, k_size):
        gate = gate + gu_in[k, 0].astype(F32)
        up = up + gu_in[k, 1].astype(F32)
    hid_own[...] = (gate / (1.0 + jnp.exp(-gate)) * up).astype(BF16)
    local[9].wait()
    sh, rh = kv_send.at[6], kv_recv.at[6]

    def hid_go(i, c):
        push("kv", lax.rem(kv + i, k_size), kv, hid_own, hid_all, sh, rh).start()
        return c

    lax.fori_loop(1, k_size, hid_go, 0)
    hid_all[kv] = hid_own[...]

    def down(i, acc):
        peer = lax.rem(kv + i, k_size)

        @pl.when(i > 0)
        def _():
            arrival("kv", peer, hid_own, hid_all, sh, rh).wait_recv()

        at = pl.ds(pl.multiple_of(peer * f_chunk, LANES), f_chunk)
        return acc + jnp.dot(hid_all[peer], wd[at, :], preferred_element_type=F32)

    y_own[...] = lax.fori_loop(0, k_size, down, jnp.zeros((seqs, width), F32))
    tp_all(2, y_own, y_in)
    z = mid.astype(F32)
    for t in range(t_size):
        z = z + y_in[t]
    wide[...] = normed(z, 7, s2_own, s2_in)
    mine = wide[:, pl.ds(pl.multiple_of(tp * LANES, LANES), LANES)]
    out[...] = (mine * gain_two[...]).astype(BF16)

    for phase, own, landing in ((0, tok_own, tok_all), (1, x_own, x_in), (2, y_own, y_in)):
        for i in range(1, t_size):
            peer = lax.rem(tp + i, t_size)
            arrival("tp", peer, own, landing, tp_send.at[phase], tp_recv.at[phase]).wait_send()

    def finish(i, c):
        peer = lax.rem(kv + i, k_size)

        @pl.when(peer < n_chunks)
        def _():
            arrival("kv", peer, qkv_part.at[peer], qkv_in, s, r).wait_send()

        @pl.when(kv < n_chunks)
        def _():
            arrival("kv", peer, qkv_own, qkv_all, s2, r2).wait_send()

        for phase, own, landing in (
            (2, att_part.at[peer], att_in),
            (3, att_own, att_all),
            (4, s1_own, s1_in),
            (5, gu_part.at[peer], gu_in),
            (6, hid_own, hid_all),
            (7, s2_own, s2_in),
        ):
            arrival("kv", peer, own, landing, kv_send.at[phase], kv_recv.at[phase]).wait_send()
        return c

    lax.fori_loop(1, k_size, finish, 0)


def fused(
    tokens,
    live_lengths,
    kv_cache,
    gate_sums,
    w_query,
    w_key,
    w_value,
    w_forget,
    forget_bias,
    w_out,
    first_gain,
    w_gate,
    w_up,
    w_down,
    second_gain,
):
    k_size, t_size = lax.axis_size("kv"), lax.axis_size("tp")
    seqs = tokens.shape[0]
    positions = kv_cache.shape[1]
    heads = kv_cache.shape[2] // (2 * DH)
    rows = heads * GROUP
    row_n, q_cols = w_query.shape
    kk = w_key.shape[1]
    width = w_out.shape[1]
    ff = w_gate.shape[1]
    chunk = kk
    n_chunks = q_cols // chunk + 3
    f_chunk = -(-ff // (k_size * LANES)) * LANES
    padded = f_chunk * k_size
    per = seqs // k_size
    dims = (seqs, k_size, t_size, heads, chunk, n_chunks, f_chunk, positions)
    vmem = pl.BlockSpec(memory_space=pltpu.VMEM)
    smem = pl.BlockSpec(memory_space=pltpu.SMEM)
    hbm = pl.BlockSpec(memory_space=pl.ANY)
    V = pltpu.VMEM
    scratch = [
        V((row_n, q_cols + 2 * kk), BF16),
        V((row_n, w_forget.shape[1]), BF16),
        V(kv_cache.shape, BF16),
        V(gate_sums.shape, F32),
        V(w_out.shape, BF16),
        V((row_n, padded), BF16),
        V((row_n, padded), BF16),
        V((padded, width), BF16),
        V((seqs + 8, LANES), F32),
        V((t_size, seqs + 8, LANES), F32),
        V((n_chunks, seqs, chunk), F32),
        V((k_size, seqs, chunk), F32),
        V((seqs, chunk), F32),
        V((k_size, seqs, chunk), F32),
        V((seqs * rows, LANES), F32),
        V((seqs * rows, LANES), F32),
        V((seqs, LANES), F32),
        V((k_size, per, rows, LANES), F32),
        V((k_size, per, rows, LANES), F32),
        V((per * rows, LANES), F32),
        V((k_size, per * rows, LANES), F32),
        V((seqs, width), F32),
        V((t_size, seqs, width), F32),
        V((seqs, width), F32),
        V((t_size, seqs, width), F32),
        V((seqs, LANES), F32),
        V((k_size, seqs, LANES), F32),
        V((seqs, LANES), F32),
        V((k_size, seqs, LANES), F32),
        V((k_size, 2, seqs, f_chunk), BF16),
        V((k_size, 2, seqs, f_chunk), BF16),
        V((seqs, f_chunk), BF16),
        V((k_size, seqs, f_chunk), BF16),
        V((seqs, width), F32),
        pltpu.SemaphoreType.DMA((10,)),
        pltpu.SemaphoreType.DMA((3, t_size)),
        pltpu.SemaphoreType.DMA((3, t_size)),
        pltpu.SemaphoreType.DMA((8, k_size)),
        pltpu.SemaphoreType.DMA((8, k_size)),
    ]
    return pl.pallas_call(
        functools.partial(fused_kernel, dims),
        out_shape=jax.ShapeDtypeStruct(tokens.shape, BF16),
        in_specs=[vmem, smem, hbm, hbm, hbm, hbm, hbm, hbm, vmem, hbm, vmem, hbm, hbm, hbm, vmem],
        out_specs=vmem,
        scratch_shapes=scratch,
        compiler_params=pltpu.CompilerParams(
            collective_id=0, has_side_effects=True, vmem_limit_bytes=60 * 1024 * 1024
        ),
    )(
        tokens,
        live_lengths,
        kv_cache,
        gate_sums,
        w_query,
        w_key,
        w_value,
        w_forget,
        forget_bias.reshape(1, -1),
        w_out,
        first_gain.reshape(1, -1),
        w_gate,
        w_up,
        w_down,
        second_gain.reshape(1, -1),
    )


def fits(tokens, kv_cache, w_query, w_key, w_gate):
    k_size = lax.axis_size("kv")
    heads = kv_cache.shape[2] // (2 * DH)
    return (
        tokens.shape[1] == LANES
        and tokens.shape[0] % 16 == 0
        and tokens.shape[0] % k_size == 0
        and heads % 2 == 0
        and w_key.shape[1] % LANES == 0
        and w_query.shape[1] % w_key.shape[1] == 0
        and w_query.shape[1] // w_key.shape[1] + 3 <= k_size
        and w_gate.shape[1] % LANES == 0
    )


def choose(*args):
    if fits(args[0], args[2], args[4], args[5], args[11]):
        return fused(*args)
    return on_device(*args)


def solution(mesh):
    in_specs = (
        P(None, ("kv", "tp")),
        P(),
        P(None, "kv", "tp"),
        P(None, "tp", "kv"),
        P("kv", "tp"),
        P("kv", "tp"),
        P("kv", "tp"),
        P(),
        P(),
        P("tp", "kv"),
        P(("kv", "tp")),
        P("kv", "tp"),
        P("kv", "tp"),
        P("tp", "kv"),
        P(("kv", "tp")),
    )
    out_specs = P(None, ("kv", "tp"))
    return jax.shard_map(
        choose, mesh=mesh, in_specs=in_specs, out_specs=out_specs, check_vma=False
    )
```

```python
import functools

import jax
import jax.numpy as jnp
from jax import lax
from jax.experimental import pallas as pl
from jax.experimental.pallas import tpu as pltpu
from jax.sharding import PartitionSpec as P

D = 4096
DH = 64
GROUP = 4


EPSILON = 1e-05
EMPTY_SCORE = -1e30


def combined_all(shard, axis, combine):
    everything = jax.tree.map(lambda part: lax.all_gather(part, axis), shard)
    initial = jax.tree.map(lambda part: part[0], everything)

    def lap(k, so_far):
        return combine(so_far, jax.tree.map(lambda part: part[k], everything))

    return lax.fori_loop(1, lax.axis_size(axis), lap, initial)


def combine_parts(earlier, later):
    earlier_top, earlier_total, earlier_sum = earlier
    later_top, later_total, later_sum = later
    joint_top = jnp.maximum(earlier_top, later_top)
    earlier_scale = jnp.exp(earlier_top - joint_top)
    later_scale = jnp.exp(later_top - joint_top)
    joint_total = earlier_total * earlier_scale + later_total * later_scale
    joint_sum = earlier_sum * earlier_scale[..., None] + later_sum * later_scale[..., None]
    return (joint_top, joint_total, joint_sum)


def normalize_block(mixture, norm_gain):
    row_sum, row_square = lax.psum(
        (jnp.sum(mixture, axis=1), jnp.sum(mixture * mixture, axis=1)), "kv"
    )
    centre = row_sum / D
    spread = row_square / D - centre * centre
    scaled = (mixture - centre[:, None]) * lax.rsqrt(spread[:, None] + EPSILON) * norm_gain
    return scaled.astype(jnp.bfloat16)


def on_device(
    tokens,
    live_lengths,
    kv_cache,
    gate_sums,
    w_query,
    w_key,
    w_value,
    w_forget,
    forget_bias,
    w_out,
    first_gain,
    w_gate,
    w_up,
    w_down,
    second_gain,
):
    sequences = tokens.shape[0]
    own_cols = tokens.shape[1]
    gains_pair = jnp.stack([first_gain, second_gain], axis=0)
    wide_rows, wide_gains = (
        lax.all_gather(tokens.astype(jnp.float32), "tp", axis=1, tiled=True),
        lax.all_gather(gains_pair, "tp", axis=1, tiled=True),
    )
    block_rows = wide_rows.astype(jnp.bfloat16)
    row_count = block_rows.shape[1]
    row_start = lax.axis_index("kv") * row_count
    local_heads = kv_cache.shape[2] // (2 * DH)
    head_start = lax.axis_index("tp") * local_heads
    forget_rows = lax.dynamic_slice(w_forget, (row_start, head_start), (row_count, local_heads))
    query_part = jnp.dot(block_rows, w_query, preferred_element_type=jnp.float32)
    key_part = jnp.dot(block_rows, w_key, preferred_element_type=jnp.float32)
    value_part = jnp.dot(block_rows, w_value, preferred_element_type=jnp.float32)
    forget_part = jnp.dot(block_rows, forget_rows, preferred_element_type=jnp.float32)
    query_sum, key_sum, value_sum, forget_sum = lax.psum(
        (query_part, key_part, value_part, forget_part), "kv"
    )
    queries = query_sum.astype(jnp.bfloat16).reshape(sequences, local_heads, GROUP, DH)
    new_keys = key_sum.astype(jnp.bfloat16).reshape(sequences, local_heads, DH)
    new_values = value_sum.astype(jnp.bfloat16).reshape(sequences, local_heads, DH)
    bias_rows = lax.dynamic_slice_in_dim(forget_bias, head_start, local_heads)
    new_gate = jax.nn.log_sigmoid(forget_sum + bias_rows)
    positions = kv_cache.shape[1]
    cached = kv_cache.reshape(sequences, positions, local_heads, 2, DH)
    score_scale = DH ** (-0.5)
    scores = (
        jnp.einsum(
            "bgjd,bpgd->bgjp", queries, cached[:, :, :, 0], preferred_element_type=jnp.float32
        )
        * score_scale
    )
    scores = scores + gate_sums[:, :, None, :] + new_gate[:, :, None, None]
    position_selector = lax.axis_index("kv") * positions + jnp.arange(positions, dtype=jnp.int32)
    live_mask = (position_selector[None, :] < live_lengths[:, None])[:, None, None, :]
    local_top = jnp.max(jnp.where(live_mask, scores, EMPTY_SCORE), axis=-1)
    weights = jnp.where(live_mask, jnp.exp(scores - local_top[..., None]), 0.0)
    local_total = jnp.sum(weights, axis=-1)
    local_sum = jnp.einsum(
        "bgjp,bpgd->bgjd",
        weights.astype(jnp.bfloat16),
        cached[:, :, :, 1],
        preferred_element_type=jnp.float32,
    )
    row_top, weight_total, summed = combined_all(
        (local_top, local_total, local_sum), "kv", combine_parts
    )
    own_score = (
        jnp.einsum("bgjd,bgd->bgj", queries, new_keys, preferred_element_type=jnp.float32)
        * score_scale
    )
    final_top = jnp.maximum(row_top, own_score)
    carry_scale = jnp.exp(row_top - final_top)
    own_weight = jnp.exp(own_score - final_top)
    own_rounded = lax.optimization_barrier(own_weight.astype(jnp.bfloat16)).astype(jnp.float32)
    numerator = summed * carry_scale[..., None] + own_rounded[..., None] * new_values[
        :, :, None, :
    ].astype(jnp.float32)
    attended = (numerator / (weight_total * carry_scale + own_weight)[..., None]).astype(
        jnp.bfloat16
    )
    attended = attended.reshape(sequences, local_heads * GROUP * DH)
    attn_part = jnp.dot(attended, w_out, preferred_element_type=jnp.float32)
    attn_block = lax.psum(attn_part, "tp")
    mid_rows = normalize_block(wide_rows + attn_block, wide_gains[0])
    gate_part = jnp.dot(mid_rows, w_gate, preferred_element_type=jnp.float32)
    up_part = jnp.dot(mid_rows, w_up, preferred_element_type=jnp.float32)
    gate_full, up_full = (
        lax.psum(gate_part.astype(jnp.bfloat16), "kv").astype(jnp.float32),
        lax.psum(up_part.astype(jnp.bfloat16), "kv").astype(jnp.float32),
    )
    hidden = (jax.nn.silu(gate_full) * up_full).astype(jnp.bfloat16)
    ffn_part = jnp.dot(hidden, w_down, preferred_element_type=jnp.float32)
    ffn_block = lax.psum(ffn_part, "tp")
    out_block = normalize_block(mid_rows.astype(jnp.float32) + ffn_block, wide_gains[1])
    return lax.dynamic_slice_in_dim(out_block, lax.axis_index("tp") * own_cols, own_cols, 1)


MESH = pl.DeviceIdType.MESH
F32 = jnp.float32
BF16 = jnp.bfloat16
LANES = 128


def push(axis, peer, me, source, landing, sends, recvs):
    return pltpu.make_async_remote_copy(
        src_ref=source,
        dst_ref=landing.at[me],
        send_sem=sends.at[peer],
        recv_sem=recvs.at[me],
        device_id={axis: peer},
        device_id_type=MESH,
    )


def partner(m, me, size):
    return lax.rem(me + 1 + m, size)


def arrival(axis, peer, source, landing, sends, recvs):
    return pltpu.make_async_remote_copy(
        src_ref=source,
        dst_ref=landing.at[peer],
        send_sem=sends.at[peer],
        recv_sem=recvs.at[peer],
        device_id={axis: peer},
        device_id_type=MESH,
    )


def head_rows(block, odd, lane):
    moved = pltpu.roll(block, DH, 1) if odd else block
    return jnp.where(lane < DH, moved, 0.0)


def fused_kernel(
    dims,
    tokens,
    lengths,
    cache_hbm,
    gates_hbm,
    wq_hbm,
    wk_hbm,
    wv_hbm,
    wf_hbm,
    bias,
    wo_hbm,
    gain_one,
    wg_hbm,
    wu_hbm,
    wd_hbm,
    gain_two,
    out,
    wqkv,
    wf,
    cache,
    gates,
    wo,
    wg,
    wu,
    wd,
    tok_own,
    tok_all,
    qkv_part,
    qkv_in,
    qkv_own,
    qkv_all,
    f_own,
    f_all,
    q_rows,
    kv_rows,
    gate_now,
    att_part,
    att_in,
    att_own,
    att_all,
    x_own,
    x_in,
    y_own,
    y_in,
    s1_own,
    s1_in,
    s2_own,
    s2_in,
    gu_part,
    gu_in,
    hid_own,
    hid_all,
    wide,
    sems,
    tp_send,
    tp_recv,
    kv_send,
    kv_recv,
):
    seqs, k_size, t_size, heads, chunk, n_chunks, f_chunk, positions = dims
    kv = lax.axis_index("kv")
    tp = lax.axis_index("tp")
    rows_n = wq_hbm.shape[0]
    q_cols = wq_hbm.shape[1]
    kk = wk_hbm.shape[1]
    ff = wg_hbm.shape[1]
    width = wo_hbm.shape[1]
    per = seqs // k_size
    rows = heads * GROUP
    local = [
        pltpu.make_async_copy(wq_hbm, wqkv.at[:, :q_cols], sems.at[0]),
        pltpu.make_async_copy(wk_hbm, wqkv.at[:, q_cols : q_cols + kk], sems.at[1]),
        pltpu.make_async_copy(wv_hbm, wqkv.at[:, q_cols + kk :], sems.at[2]),
        pltpu.make_async_copy(
            wf_hbm.at[:, pl.ds(pl.multiple_of(kv * rows_n, rows_n), rows_n)], wf, sems.at[3]
        ),
        pltpu.make_async_copy(cache_hbm, cache, sems.at[4]),
        pltpu.make_async_copy(gates_hbm, gates, sems.at[5]),
        pltpu.make_async_copy(wo_hbm, wo, sems.at[6]),
        pltpu.make_async_copy(wg_hbm, wg.at[:, :ff], sems.at[7]),
        pltpu.make_async_copy(wu_hbm, wu.at[:, :ff], sems.at[8]),
        pltpu.make_async_copy(wd_hbm, wd.at[:ff, :], sems.at[9]),
    ]
    barrier = pltpu.get_barrier_semaphore()
    for i in range(k_size - 1):
        pl.semaphore_signal(
            barrier, inc=1, device_id={"kv": partner(i, kv, k_size)}, device_id_type=MESH
        )
    for i in range(1, t_size):
        pl.semaphore_signal(
            barrier, inc=1, device_id={"tp": lax.rem(tp + i, t_size)}, device_id_type=MESH
        )
    for copy in local:
        copy.start()
    padded = wg.shape[1]
    if padded > ff:
        wg[:, ff:] = jnp.zeros((rows_n, padded - ff), BF16)
        wu[:, ff:] = jnp.zeros((rows_n, padded - ff), BF16)
        wd[ff:, :] = jnp.zeros((padded - ff, width), BF16)
    tok_own[:seqs, :] = tokens[...].astype(F32)
    tok_own[seqs:, :] = jnp.broadcast_to(gain_one[...], (8, LANES))
    pl.semaphore_wait(barrier, k_size - 1 + t_size - 1)

    def tp_all(phase, own, landing):
        s, r = tp_send.at[phase], tp_recv.at[phase]
        for i in range(1, t_size):
            push("tp", lax.rem(tp + i, t_size), tp, own, landing, s, r).start()
        landing[tp] = own[...]
        for i in range(1, t_size):
            arrival("tp", lax.rem(tp + i, t_size), own, landing, s, r).wait_recv()

    def kv_all(phase, own, landing):
        s, r = kv_send.at[phase], kv_recv.at[phase]

        def go(i, c):
            push("kv", partner(i, kv, k_size), kv, own, landing, s, r).start()
            return c

        def come(i, c):
            arrival("kv", partner(i, kv, k_size), own, landing, s, r).wait_recv()
            return c

        lax.fori_loop(0, k_size - 1, go, 0)
        landing[kv] = own[...]
        lax.fori_loop(0, k_size - 1, come, 0)

    tp_all(0, tok_own, tok_all)
    wide_rows = jnp.concatenate([tok_all[t, :seqs, :] for t in range(t_size)], axis=1)
    wide_gain = jnp.concatenate([tok_all[t, seqs : seqs + 1, :] for t in range(t_size)], axis=1)
    wide[...] = wide_rows
    block = wide_rows.astype(BF16)
    for n in range(4):
        local[n].wait()
    for c in range(n_chunks - 1):
        qkv_part[c] = jnp.dot(
            block, wqkv[:, c * chunk : (c + 1) * chunk], preferred_element_type=F32
        )
    kv_heads = wf.shape[0]
    qkv_part[n_chunks - 1] = jnp.zeros((seqs, chunk), F32)
    qkv_part[n_chunks - 1, :, :kv_heads] = lax.dot_general(
        block, wf[...], (((1,), (1,)), ((), ())), preferred_element_type=F32
    )
    s, r = kv_send.at[0], kv_recv.at[0]
    s2, r2 = kv_send.at[1], kv_recv.at[1]

    def qkv_go(i, c):
        peer = partner(i, kv, k_size)

        @pl.when(peer < n_chunks)
        def _():
            push("kv", peer, kv, qkv_part.at[peer], qkv_in, s, r).start()

        return c

    lax.fori_loop(0, k_size - 1, qkv_go, 0)

    @pl.when(kv < n_chunks)
    def _():
        qkv_in[kv] = qkv_part[kv]

        def come(i, c):
            peer = partner(i, kv, k_size)
            arrival("kv", peer, qkv_part.at[0], qkv_in, s, r).wait_recv()
            return c

        lax.fori_loop(0, k_size - 1, come, 0)
        total = qkv_in[0]
        for k in range(1, k_size):
            total = total + qkv_in[k]
        scale = jnp.where(kv < q_cols // chunk, DH**-0.5, 1.0).astype(F32)
        qkv_own[...] = (total.astype(BF16).astype(F32) * scale).astype(BF16)
        f_own[...] = total[:, :LANES]

        @pl.when(kv < n_chunks - 1)
        def _():
            def go(i, c):
                push("kv", partner(i, kv, k_size), kv, qkv_own, qkv_all, s2, r2).start()
                return c

            lax.fori_loop(0, k_size - 1, go, 0)
            qkv_all[kv] = qkv_own[...]

        @pl.when(kv == n_chunks - 1)
        def _():
            def go(i, c):
                push("kv", partner(i, kv, k_size), kv, f_own, f_all, s2, r2).start()
                return c

            lax.fori_loop(0, k_size - 1, go, 0)
            f_all[kv] = f_own[...]

    def qkv_come(i, c):
        peer = partner(i, kv, k_size)

        @pl.when(peer < n_chunks - 1)
        def _():
            arrival("kv", peer, qkv_own, qkv_all, s2, r2).wait_recv()

        @pl.when(peer == n_chunks - 1)
        def _():
            arrival("kv", peer, f_own, f_all, s2, r2).wait_recv()

        return c

    lax.fori_loop(0, k_size - 1, qkv_come, 0)
    lane = lax.broadcasted_iota(jnp.int32, (seqs, LANES), 1)

    def unit(start):
        return qkv_all[start // chunk, :, start % chunk : start % chunk + LANES].astype(F32)

    for h in range(rows):
        start = h * DH
        base = start // LANES * LANES
        q_rows[pl.ds(h, seqs, stride=rows), :] = head_rows(unit(base), start % LANES != 0, lane)
    for g in range(heads):
        base = g * DH // LANES * LANES
        odd = g % 2 == 1
        keys = unit(q_cols + base)
        values = unit(q_cols + kk + base)
        keys = pltpu.roll(keys, DH, 1) if odd else keys
        values = values if odd else pltpu.roll(values, DH, 1)
        pair = jnp.where(lane < DH, keys, values)
        for j in range(GROUP):
            kv_rows[pl.ds(g * GROUP + j, seqs, stride=rows), :] = pair
    logits = f_all[n_chunks - 1, :, :kv_heads] + bias[...]
    gate_now[:, :kv_heads] = jnp.minimum(logits, 0.0) - jnp.log(1.0 + jnp.exp(-jnp.abs(logits)))
    local[4].wait()
    local[5].wait()
    row_p = lax.broadcasted_iota(jnp.int32, (rows, positions), 0) // GROUP
    pos = lax.broadcasted_iota(jnp.int32, (rows, positions), 1) + kv * positions
    row_l = lax.broadcasted_iota(jnp.int32, (rows, LANES), 0) // GROUP
    lane_l = lax.broadcasted_iota(jnp.int32, (rows, LANES), 1)
    row_g = lax.broadcasted_iota(jnp.int32, (rows, kv_heads), 0) // GROUP
    lane_g = lax.broadcasted_iota(jnp.int32, (rows, kv_heads), 1)

    def attend(b):
        q = q_rows[pl.ds(pl.multiple_of(b * rows, rows), rows), :]
        spread = jnp.concatenate(
            [jnp.where(row_l == g, q, 0.0).astype(BF16) for g in range(heads)], axis=1
        )
        slab = cache[b]
        scores = lax.dot_general(
            spread, slab, (((1,), (1,)), ((), ())), preferred_element_type=F32
        )
        gate_rows = gates[b]
        gate = jnp.broadcast_to(gate_rows[0:1], (rows, positions))
        for g in range(1, heads):
            gate = jnp.where(row_p == g, gate_rows[g : g + 1], gate)
        fresh = jnp.sum(
            jnp.where(lane_g == row_g + tp * heads, gate_now[pl.ds(b, 1), :kv_heads], 0.0),
            axis=1,
            keepdims=True,
        )
        scores = scores + gate + fresh
        live = pos < lengths[b]
        scores = jnp.where(live, scores, EMPTY_SCORE)
        top = jnp.max(scores, axis=1, keepdims=True)
        weights = jnp.where(live, jnp.exp(scores - top), 0.0)
        total = jnp.sum(weights, axis=1, keepdims=True)
        mixed = jnp.dot(weights.astype(BF16), slab, preferred_element_type=F32)
        own = mixed[:, :LANES]
        for g in range(1, heads):
            own = jnp.where(row_l == g, mixed[:, g * LANES : (g + 1) * LANES], own)
        own = jnp.where(lane_l < DH // 2, top, jnp.where(lane_l < DH, total, own))
        return own

    sa, ra = kv_send.at[2], kv_recv.at[2]

    def att_go(i, c):
        peer = partner(i, kv, k_size)
        for e in range(per):
            att_part[peer, e] = attend(peer * per + e)

        @pl.when(i < k_size - 1)
        def _():
            push("kv", peer, kv, att_part.at[peer], att_in, sa, ra).start()

        return c

    lax.fori_loop(0, k_size, att_go, 0)
    att_in[kv] = att_part[kv]

    def att_come(i, c):
        arrival("kv", partner(i, kv, k_size), att_part.at[0], att_in, sa, ra).wait_recv()
        return c

    lax.fori_loop(0, k_size - 1, att_come, 0)
    for e in range(per):
        at = pl.ds(pl.multiple_of((kv * per + e) * rows, rows), rows)
        q, pair = q_rows[at, :], kv_rows[at, :]
        own_score = jnp.sum(jnp.where(lane_l < DH, q * pair, 0.0), axis=1, keepdims=True)
        parts = [att_in[k, e] for k in range(k_size)]
        tops = [part[:, 0:1] for part in parts]
        high = own_score
        for top in tops:
            high = jnp.maximum(high, top)
        own_weight = jnp.exp(own_score - high)
        numer = own_weight.astype(BF16).astype(F32) * pair
        denom = own_weight
        for top, part in zip(tops, parts):
            scale = jnp.exp(top - high)
            numer = numer + part * scale
            denom = denom + part[:, DH // 2 : DH // 2 + 1] * scale
        done = numer / denom
        if e % 2 == 0:
            left = pltpu.roll(done, DH, 1)
        else:
            both = jnp.where(lane_l < DH, left, done).astype(BF16)
            att_own[e // 2 * rows : (e // 2 + 1) * rows, :] = both
    kv_all(3, att_own, att_all)
    for k in range(k_size):
        for e in range(per):
            pair = att_all[k, e // 2 * rows : (e // 2 + 1) * rows, :].astype(F32)
            pair = pltpu.roll(pair, DH, 1) if e % 2 == 0 else pair
            q_rows[(k * per + e) * rows : (k * per + e + 1) * rows, :] = pair
    pieces = []
    for h in range(0, rows, 2):
        even = pltpu.roll(q_rows[pl.ds(h, seqs, stride=rows), :], DH, 1)
        odd = q_rows[pl.ds(h + 1, seqs, stride=rows), :]
        pieces.append(jnp.where(lane < DH, even, odd).astype(BF16))
    attended = jnp.concatenate(pieces, axis=1)
    local[6].wait()
    x_own[...] = jnp.dot(attended, wo[...], preferred_element_type=F32)

    def normed(z, phase, stat_own, stat_in):
        row_sum = jnp.sum(z, axis=1, keepdims=True)
        row_square = jnp.sum(z * z, axis=1, keepdims=True)
        stat_own[...] = jnp.where(lane == 0, row_sum, row_square)
        kv_all(phase, stat_own, stat_in)
        stats = stat_in[0]
        for k in range(1, k_size):
            stats = stats + stat_in[k]
        count = k_size * width
        centre = stats[:, 0:1] / count
        spread = stats[:, 1:2] / count - centre * centre
        return (z - centre) * lax.rsqrt(spread + EPSILON)

    tp_all(1, x_own, x_in)
    z = wide[...]
    for t in range(t_size):
        z = z + x_in[t]
    mid = (normed(z, 4, s1_own, s1_in) * wide_gain).astype(BF16)
    local[7].wait()
    local[8].wait()
    sg, rg = kv_send.at[5], kv_recv.at[5]

    def gu_go(i, c):
        peer = partner(i, kv, k_size)
        at = pl.ds(pl.multiple_of(peer * f_chunk, LANES), f_chunk)
        gu_part[peer, 0] = jnp.dot(mid, wg[:, at], preferred_element_type=F32).astype(BF16)
        gu_part[peer, 1] = jnp.dot(mid, wu[:, at], preferred_element_type=F32).astype(BF16)

        @pl.when(i < k_size - 1)
        def _():
            push("kv", peer, kv, gu_part.at[peer], gu_in, sg, rg).start()

        return c

    lax.fori_loop(0, k_size, gu_go, 0)
    gu_in[kv] = gu_part[kv]

    def gu_come(i, c):
        arrival("kv", partner(i, kv, k_size), gu_part.at[0], gu_in, sg, rg).wait_recv()
        return c

    lax.fori_loop(0, k_size - 1, gu_come, 0)
    gate = gu_in[0, 0].astype(F32)
    up = gu_in[0, 1].astype(F32)
    for k in range(1, k_size):
        gate = gate + gu_in[k, 0].astype(F32)
        up = up + gu_in[k, 1].astype(F32)
    hid_own[...] = (gate / (1.0 + jnp.exp(-gate)) * up).astype(BF16)
    local[9].wait()
    sh, rh = kv_send.at[6], kv_recv.at[6]

    def hid_go(i, c):
        push("kv", partner(i, kv, k_size), kv, hid_own, hid_all, sh, rh).start()
        return c

    lax.fori_loop(0, k_size - 1, hid_go, 0)
    hid_all[kv] = hid_own[...]

    def down(i, acc):
        peer = lax.rem(kv + i, k_size)

        @pl.when(i > 0)
        def _():
            arrival("kv", peer, hid_own, hid_all, sh, rh).wait_recv()

        at = pl.ds(pl.multiple_of(peer * f_chunk, LANES), f_chunk)
        return acc + jnp.dot(hid_all[peer], wd[at, :], preferred_element_type=F32)

    y_own[...] = lax.fori_loop(0, k_size, down, jnp.zeros((seqs, width), F32))
    tp_all(2, y_own, y_in)
    z = mid.astype(F32)
    for t in range(t_size):
        z = z + y_in[t]
    wide[...] = normed(z, 7, s2_own, s2_in)
    mine = wide[:, pl.ds(pl.multiple_of(tp * LANES, LANES), LANES)]
    out[...] = (mine * gain_two[...]).astype(BF16)

    for phase, own, landing in ((0, tok_own, tok_all), (1, x_own, x_in), (2, y_own, y_in)):
        for i in range(1, t_size):
            peer = lax.rem(tp + i, t_size)
            arrival("tp", peer, own, landing, tp_send.at[phase], tp_recv.at[phase]).wait_send()

    def finish(i, c):
        peer = partner(i, kv, k_size)

        @pl.when(peer < n_chunks)
        def _():
            arrival("kv", peer, qkv_part.at[peer], qkv_in, s, r).wait_send()

        @pl.when(kv < n_chunks - 1)
        def _():
            arrival("kv", peer, qkv_own, qkv_all, s2, r2).wait_send()

        @pl.when(kv == n_chunks - 1)
        def _():
            arrival("kv", peer, f_own, f_all, s2, r2).wait_send()

        for phase, own, landing in (
            (2, att_part.at[peer], att_in),
            (3, att_own, att_all),
            (4, s1_own, s1_in),
            (5, gu_part.at[peer], gu_in),
            (6, hid_own, hid_all),
            (7, s2_own, s2_in),
        ):
            arrival("kv", peer, own, landing, kv_send.at[phase], kv_recv.at[phase]).wait_send()
        return c

    lax.fori_loop(0, k_size - 1, finish, 0)


def fused(
    tokens,
    live_lengths,
    kv_cache,
    gate_sums,
    w_query,
    w_key,
    w_value,
    w_forget,
    forget_bias,
    w_out,
    first_gain,
    w_gate,
    w_up,
    w_down,
    second_gain,
):
    k_size, t_size = lax.axis_size("kv"), lax.axis_size("tp")
    seqs = tokens.shape[0]
    positions = kv_cache.shape[1]
    heads = kv_cache.shape[2] // (2 * DH)
    rows = heads * GROUP
    row_n, q_cols = w_query.shape
    kk = w_key.shape[1]
    width = w_out.shape[1]
    ff = w_gate.shape[1]
    chunk = kk
    n_chunks = q_cols // chunk + 3
    f_chunk = -(-ff // (k_size * LANES)) * LANES
    padded = f_chunk * k_size
    per = seqs // k_size
    dims = (seqs, k_size, t_size, heads, chunk, n_chunks, f_chunk, positions)
    vmem = pl.BlockSpec(memory_space=pltpu.VMEM)
    smem = pl.BlockSpec(memory_space=pltpu.SMEM)
    hbm = pl.BlockSpec(memory_space=pl.ANY)
    V = pltpu.VMEM
    scratch = [
        V((row_n, q_cols + 2 * kk), BF16),
        V((w_forget.shape[1], row_n), BF16),
        V(kv_cache.shape, BF16),
        V(gate_sums.shape, F32),
        V(w_out.shape, BF16),
        V((row_n, padded), BF16),
        V((row_n, padded), BF16),
        V((padded, width), BF16),
        V((seqs + 8, LANES), F32),
        V((t_size, seqs + 8, LANES), F32),
        V((n_chunks, seqs, chunk), F32),
        V((k_size, seqs, chunk), F32),
        V((seqs, chunk), BF16),
        V((k_size, seqs, chunk), BF16),
        V((seqs, LANES), F32),
        V((k_size, seqs, LANES), F32),
        V((seqs * rows, LANES), F32),
        V((seqs * rows, LANES), F32),
        V((seqs, LANES), F32),
        V((k_size, per, rows, LANES), F32),
        V((k_size, per, rows, LANES), F32),
        V((per // 2 * rows, LANES), BF16),
        V((k_size, per // 2 * rows, LANES), BF16),
        V((seqs, width), F32),
        V((t_size, seqs, width), F32),
        V((seqs, width), F32),
        V((t_size, seqs, width), F32),
        V((seqs, LANES), F32),
        V((k_size, seqs, LANES), F32),
        V((seqs, LANES), F32),
        V((k_size, seqs, LANES), F32),
        V((k_size, 2, seqs, f_chunk), BF16),
        V((k_size, 2, seqs, f_chunk), BF16),
        V((seqs, f_chunk), BF16),
        V((k_size, seqs, f_chunk), BF16),
        V((seqs, width), F32),
        pltpu.SemaphoreType.DMA((10,)),
        pltpu.SemaphoreType.DMA((3, t_size)),
        pltpu.SemaphoreType.DMA((3, t_size)),
        pltpu.SemaphoreType.DMA((8, k_size)),
        pltpu.SemaphoreType.DMA((8, k_size)),
    ]
    return pl.pallas_call(
        functools.partial(fused_kernel, dims),
        out_shape=jax.ShapeDtypeStruct(tokens.shape, BF16),
        in_specs=[vmem, smem, hbm, hbm, hbm, hbm, hbm, hbm, vmem, hbm, vmem, hbm, hbm, hbm, vmem],
        out_specs=vmem,
        scratch_shapes=scratch,
        compiler_params=pltpu.CompilerParams(
            collective_id=0, has_side_effects=True, vmem_limit_bytes=60 * 1024 * 1024
        ),
    )(
        tokens,
        live_lengths,
        kv_cache,
        gate_sums,
        w_query,
        w_key,
        w_value,
        w_forget.T,
        forget_bias.reshape(1, -1),
        w_out,
        first_gain.reshape(1, -1),
        w_gate,
        w_up,
        w_down,
        second_gain.reshape(1, -1),
    )


def fits(tokens, kv_cache, w_query, w_key, w_gate):
    k_size = lax.axis_size("kv")
    heads = kv_cache.shape[2] // (2 * DH)
    return (
        tokens.shape[1] == LANES
        and tokens.shape[0] % 16 == 0
        and tokens.shape[0] % (2 * k_size) == 0
        and k_size % 2 == 0
        and heads % 2 == 0
        and w_key.shape[1] % LANES == 0
        and w_query.shape[1] % w_key.shape[1] == 0
        and w_query.shape[1] // w_key.shape[1] + 3 <= k_size
        and w_gate.shape[1] % LANES == 0
    )


def choose(*args):
    if fits(args[0], args[2], args[4], args[5], args[11]):
        return fused(*args)
    return on_device(*args)


def solution(mesh):
    in_specs = (
        P(None, ("kv", "tp")),
        P(),
        P(None, "kv", "tp"),
        P(None, "tp", "kv"),
        P("kv", "tp"),
        P("kv", "tp"),
        P("kv", "tp"),
        P(),
        P(),
        P("tp", "kv"),
        P(("kv", "tp")),
        P("kv", "tp"),
        P("kv", "tp"),
        P("tp", "kv"),
        P(("kv", "tp")),
    )
    out_specs = P(None, ("kv", "tp"))
    return jax.shard_map(
        choose, mesh=mesh, in_specs=in_specs, out_specs=out_specs, check_vma=False
    )
```

```python
import functools

import jax
import jax.numpy as jnp
from jax import lax
from jax.experimental import pallas as pl
from jax.experimental.pallas import tpu as pltpu
from jax.sharding import PartitionSpec as P

D = 4096
DH = 64
GROUP = 4


EPSILON = 1e-05
EMPTY_SCORE = -1e30


def combined_all(shard, axis, combine):
    everything = jax.tree.map(lambda part: lax.all_gather(part, axis), shard)
    initial = jax.tree.map(lambda part: part[0], everything)

    def lap(k, so_far):
        return combine(so_far, jax.tree.map(lambda part: part[k], everything))

    return lax.fori_loop(1, lax.axis_size(axis), lap, initial)


def combine_parts(earlier, later):
    earlier_top, earlier_total, earlier_sum = earlier
    later_top, later_total, later_sum = later
    joint_top = jnp.maximum(earlier_top, later_top)
    earlier_scale = jnp.exp(earlier_top - joint_top)
    later_scale = jnp.exp(later_top - joint_top)
    joint_total = earlier_total * earlier_scale + later_total * later_scale
    joint_sum = earlier_sum * earlier_scale[..., None] + later_sum * later_scale[..., None]
    return (joint_top, joint_total, joint_sum)


def normalize_block(mixture, norm_gain):
    row_sum, row_square = lax.psum(
        (jnp.sum(mixture, axis=1), jnp.sum(mixture * mixture, axis=1)), "kv"
    )
    centre = row_sum / D
    spread = row_square / D - centre * centre
    scaled = (mixture - centre[:, None]) * lax.rsqrt(spread[:, None] + EPSILON) * norm_gain
    return scaled.astype(jnp.bfloat16)


def on_device(
    tokens,
    live_lengths,
    kv_cache,
    gate_sums,
    w_query,
    w_key,
    w_value,
    w_forget,
    forget_bias,
    w_out,
    first_gain,
    w_gate,
    w_up,
    w_down,
    second_gain,
):
    sequences = tokens.shape[0]
    own_cols = tokens.shape[1]
    gains_pair = jnp.stack([first_gain, second_gain], axis=0)
    wide_rows, wide_gains = (
        lax.all_gather(tokens.astype(jnp.float32), "tp", axis=1, tiled=True),
        lax.all_gather(gains_pair, "tp", axis=1, tiled=True),
    )
    block_rows = wide_rows.astype(jnp.bfloat16)
    row_count = block_rows.shape[1]
    row_start = lax.axis_index("kv") * row_count
    local_heads = kv_cache.shape[2] // (2 * DH)
    head_start = lax.axis_index("tp") * local_heads
    forget_rows = lax.dynamic_slice(w_forget, (row_start, head_start), (row_count, local_heads))
    query_part = jnp.dot(block_rows, w_query, preferred_element_type=jnp.float32)
    key_part = jnp.dot(block_rows, w_key, preferred_element_type=jnp.float32)
    value_part = jnp.dot(block_rows, w_value, preferred_element_type=jnp.float32)
    forget_part = jnp.dot(block_rows, forget_rows, preferred_element_type=jnp.float32)
    query_sum, key_sum, value_sum, forget_sum = lax.psum(
        (query_part, key_part, value_part, forget_part), "kv"
    )
    queries = query_sum.astype(jnp.bfloat16).reshape(sequences, local_heads, GROUP, DH)
    new_keys = key_sum.astype(jnp.bfloat16).reshape(sequences, local_heads, DH)
    new_values = value_sum.astype(jnp.bfloat16).reshape(sequences, local_heads, DH)
    bias_rows = lax.dynamic_slice_in_dim(forget_bias, head_start, local_heads)
    new_gate = jax.nn.log_sigmoid(forget_sum + bias_rows)
    positions = kv_cache.shape[1]
    cached = kv_cache.reshape(sequences, positions, local_heads, 2, DH)
    score_scale = DH ** (-0.5)
    scores = (
        jnp.einsum(
            "bgjd,bpgd->bgjp", queries, cached[:, :, :, 0], preferred_element_type=jnp.float32
        )
        * score_scale
    )
    scores = scores + gate_sums[:, :, None, :] + new_gate[:, :, None, None]
    position_selector = lax.axis_index("kv") * positions + jnp.arange(positions, dtype=jnp.int32)
    live_mask = (position_selector[None, :] < live_lengths[:, None])[:, None, None, :]
    local_top = jnp.max(jnp.where(live_mask, scores, EMPTY_SCORE), axis=-1)
    weights = jnp.where(live_mask, jnp.exp(scores - local_top[..., None]), 0.0)
    local_total = jnp.sum(weights, axis=-1)
    local_sum = jnp.einsum(
        "bgjp,bpgd->bgjd",
        weights.astype(jnp.bfloat16),
        cached[:, :, :, 1],
        preferred_element_type=jnp.float32,
    )
    row_top, weight_total, summed = combined_all(
        (local_top, local_total, local_sum), "kv", combine_parts
    )
    own_score = (
        jnp.einsum("bgjd,bgd->bgj", queries, new_keys, preferred_element_type=jnp.float32)
        * score_scale
    )
    final_top = jnp.maximum(row_top, own_score)
    carry_scale = jnp.exp(row_top - final_top)
    own_weight = jnp.exp(own_score - final_top)
    own_rounded = lax.optimization_barrier(own_weight.astype(jnp.bfloat16)).astype(jnp.float32)
    numerator = summed * carry_scale[..., None] + own_rounded[..., None] * new_values[
        :, :, None, :
    ].astype(jnp.float32)
    attended = (numerator / (weight_total * carry_scale + own_weight)[..., None]).astype(
        jnp.bfloat16
    )
    attended = attended.reshape(sequences, local_heads * GROUP * DH)
    attn_part = jnp.dot(attended, w_out, preferred_element_type=jnp.float32)
    attn_block = lax.psum(attn_part, "tp")
    mid_rows = normalize_block(wide_rows + attn_block, wide_gains[0])
    gate_part = jnp.dot(mid_rows, w_gate, preferred_element_type=jnp.float32)
    up_part = jnp.dot(mid_rows, w_up, preferred_element_type=jnp.float32)
    gate_full, up_full = (
        lax.psum(gate_part.astype(jnp.bfloat16), "kv").astype(jnp.float32),
        lax.psum(up_part.astype(jnp.bfloat16), "kv").astype(jnp.float32),
    )
    hidden = (jax.nn.silu(gate_full) * up_full).astype(jnp.bfloat16)
    ffn_part = jnp.dot(hidden, w_down, preferred_element_type=jnp.float32)
    ffn_block = lax.psum(ffn_part, "tp")
    out_block = normalize_block(mid_rows.astype(jnp.float32) + ffn_block, wide_gains[1])
    return lax.dynamic_slice_in_dim(out_block, lax.axis_index("tp") * own_cols, own_cols, 1)


MESH = pl.DeviceIdType.MESH
F32 = jnp.float32
BF16 = jnp.bfloat16
LANES = 128


def push(axis, peer, me, source, landing, sends, recvs):
    return pltpu.make_async_remote_copy(
        src_ref=source,
        dst_ref=landing.at[me],
        send_sem=sends.at[peer],
        recv_sem=recvs.at[me],
        device_id={axis: peer},
        device_id_type=MESH,
    )


def partner(m, me, size):
    return lax.rem(me + 1 + m, size)


def arrival(axis, peer, source, landing, sends, recvs):
    return pltpu.make_async_remote_copy(
        src_ref=source,
        dst_ref=landing.at[peer],
        send_sem=sends.at[peer],
        recv_sem=recvs.at[peer],
        device_id={axis: peer},
        device_id_type=MESH,
    )


def head_rows(block, odd, lane):
    moved = pltpu.roll(block, DH, 1) if odd else block
    return jnp.where(lane < DH, moved, 0.0)


def fused_kernel(
    dims,
    tokens,
    lengths,
    cache_hbm,
    gates_hbm,
    wq_hbm,
    wk_hbm,
    wv_hbm,
    wf_hbm,
    bias,
    wo_hbm,
    gain_one,
    wg_hbm,
    wu_hbm,
    wd_hbm,
    gain_two,
    out,
    wqkv,
    wf,
    cache,
    gates,
    wo,
    wg,
    wu,
    wd,
    tok_own,
    tok_all,
    qkv_part,
    qkv_in,
    qkv_own,
    qkv_all,
    f_own,
    f_all,
    q_rows,
    kv_rows,
    gate_now,
    att_part,
    att_in,
    att_own,
    att_all,
    x_own,
    x_in,
    y_own,
    y_in,
    s1_own,
    s1_in,
    s2_own,
    s2_in,
    gu_part,
    gu_in,
    g_part,
    g_in,
    hid_own,
    hid_all,
    wide,
    sems,
    tp_send,
    tp_recv,
    kv_send,
    kv_recv,
):
    seqs, k_size, t_size, heads, chunk, n_chunks, f_chunk, positions = dims
    kv = lax.axis_index("kv")
    tp = lax.axis_index("tp")
    rows_n = wq_hbm.shape[0]
    q_cols = wq_hbm.shape[1]
    kk = wk_hbm.shape[1]
    ff = wg_hbm.shape[1]
    width = wo_hbm.shape[1]
    per = seqs // k_size
    rows = heads * GROUP
    local = [
        pltpu.make_async_copy(wq_hbm, wqkv.at[:, :q_cols], sems.at[0]),
        pltpu.make_async_copy(wk_hbm, wqkv.at[:, q_cols : q_cols + kk], sems.at[1]),
        pltpu.make_async_copy(wv_hbm, wqkv.at[:, q_cols + kk :], sems.at[2]),
        pltpu.make_async_copy(
            wf_hbm.at[:, pl.ds(pl.multiple_of(kv * rows_n, rows_n), rows_n)], wf, sems.at[3]
        ),
        pltpu.make_async_copy(cache_hbm, cache, sems.at[4]),
        pltpu.make_async_copy(gates_hbm, gates, sems.at[5]),
        pltpu.make_async_copy(wo_hbm, wo, sems.at[6]),
        pltpu.make_async_copy(wg_hbm, wg.at[:, :ff], sems.at[7]),
        pltpu.make_async_copy(wu_hbm, wu.at[:, :ff], sems.at[8]),
        pltpu.make_async_copy(wd_hbm, wd.at[:ff, :], sems.at[9]),
    ]
    barrier = pltpu.get_barrier_semaphore()
    for i in range(k_size - 1):
        pl.semaphore_signal(
            barrier, inc=1, device_id={"kv": partner(i, kv, k_size)}, device_id_type=MESH
        )
    for i in range(1, t_size):
        pl.semaphore_signal(
            barrier, inc=1, device_id={"tp": lax.rem(tp + i, t_size)}, device_id_type=MESH
        )
    for copy in local:
        copy.start()
    padded = wg.shape[1]
    if padded > ff:
        wg[:, ff:] = jnp.zeros((rows_n, padded - ff), BF16)
        wu[:, ff:] = jnp.zeros((rows_n, padded - ff), BF16)
        wd[ff:, :] = jnp.zeros((padded - ff, width), BF16)
    tok_own[:seqs, :] = tokens[...].astype(F32)
    tok_own[seqs:, :] = jnp.broadcast_to(gain_one[...], (8, LANES))
    pl.semaphore_wait(barrier, k_size - 1 + t_size - 1)

    def tp_all(phase, own, landing):
        s, r = tp_send.at[phase], tp_recv.at[phase]
        for i in range(1, t_size):
            push("tp", lax.rem(tp + i, t_size), tp, own, landing, s, r).start()
        landing[tp] = own[...]
        for i in range(1, t_size):
            arrival("tp", lax.rem(tp + i, t_size), own, landing, s, r).wait_recv()

    def kv_all(phase, own, landing):
        s, r = kv_send.at[phase], kv_recv.at[phase]

        def go(i, c):
            push("kv", partner(i, kv, k_size), kv, own, landing, s, r).start()
            return c

        def come(i, c):
            arrival("kv", partner(i, kv, k_size), own, landing, s, r).wait_recv()
            return c

        lax.fori_loop(0, k_size - 1, go, 0)
        landing[kv] = own[...]
        lax.fori_loop(0, k_size - 1, come, 0)

    tp_all(0, tok_own, tok_all)
    wide_rows = jnp.concatenate([tok_all[t, :seqs, :] for t in range(t_size)], axis=1)
    wide_gain = jnp.concatenate([tok_all[t, seqs : seqs + 1, :] for t in range(t_size)], axis=1)
    wide[...] = wide_rows
    block = wide_rows.astype(BF16)
    for n in range(4):
        local[n].wait()
    for c in range(n_chunks - 1):
        qkv_part[c] = jnp.dot(
            block, wqkv[:, c * chunk : (c + 1) * chunk], preferred_element_type=F32
        )
    kv_heads = wf.shape[0]
    qkv_part[n_chunks - 1] = jnp.zeros((seqs, chunk), F32)
    qkv_part[n_chunks - 1, :, :kv_heads] = lax.dot_general(
        block, wf[...], (((1,), (1,)), ((), ())), preferred_element_type=F32
    )
    s, r = kv_send.at[0], kv_recv.at[0]
    s2, r2 = kv_send.at[1], kv_recv.at[1]

    def qkv_go(i, c):
        peer = partner(i, kv, k_size)

        @pl.when(peer < n_chunks)
        def _():
            push("kv", peer, kv, qkv_part.at[peer], qkv_in, s, r).start()

        return c

    lax.fori_loop(0, k_size - 1, qkv_go, 0)

    @pl.when(kv < n_chunks)
    def _():
        qkv_in[kv] = qkv_part[kv]

        def come(i, c):
            peer = partner(i, kv, k_size)
            arrival("kv", peer, qkv_part.at[0], qkv_in, s, r).wait_recv()
            return c

        lax.fori_loop(0, k_size - 1, come, 0)
        total = qkv_in[0]
        for k in range(1, k_size):
            total = total + qkv_in[k]
        scale = jnp.where(kv < q_cols // chunk, DH**-0.5, 1.0).astype(F32)
        qkv_own[...] = (total.astype(BF16).astype(F32) * scale).astype(BF16)
        f_own[...] = total[:, :LANES]

        @pl.when(kv < n_chunks - 1)
        def _():
            def go(i, c):
                push("kv", partner(i, kv, k_size), kv, qkv_own, qkv_all, s2, r2).start()
                return c

            lax.fori_loop(0, k_size - 1, go, 0)
            qkv_all[kv] = qkv_own[...]

        @pl.when(kv == n_chunks - 1)
        def _():
            def go(i, c):
                push("kv", partner(i, kv, k_size), kv, f_own, f_all, s2, r2).start()
                return c

            lax.fori_loop(0, k_size - 1, go, 0)
            f_all[kv] = f_own[...]

    def qkv_come(i, c):
        peer = partner(i, kv, k_size)

        @pl.when(peer < n_chunks - 1)
        def _():
            arrival("kv", peer, qkv_own, qkv_all, s2, r2).wait_recv()

        @pl.when(peer == n_chunks - 1)
        def _():
            arrival("kv", peer, f_own, f_all, s2, r2).wait_recv()

        return c

    lax.fori_loop(0, k_size - 1, qkv_come, 0)
    lane = lax.broadcasted_iota(jnp.int32, (seqs, LANES), 1)

    def unit(start):
        return qkv_all[start // chunk, :, start % chunk : start % chunk + LANES].astype(F32)

    for h in range(rows):
        start = h * DH
        base = start // LANES * LANES
        q_rows[pl.ds(h, seqs, stride=rows), :] = head_rows(unit(base), start % LANES != 0, lane)
    for g in range(heads):
        base = g * DH // LANES * LANES
        odd = g % 2 == 1
        keys = unit(q_cols + base)
        values = unit(q_cols + kk + base)
        keys = pltpu.roll(keys, DH, 1) if odd else keys
        values = values if odd else pltpu.roll(values, DH, 1)
        pair = jnp.where(lane < DH, keys, values)
        for j in range(GROUP):
            kv_rows[pl.ds(g * GROUP + j, seqs, stride=rows), :] = pair
    logits = f_all[n_chunks - 1, :, :kv_heads] + bias[...]
    gate_now[:, :kv_heads] = jnp.minimum(logits, 0.0) - jnp.log(1.0 + jnp.exp(-jnp.abs(logits)))
    local[4].wait()
    local[5].wait()
    row_p = lax.broadcasted_iota(jnp.int32, (rows, positions), 0) // GROUP
    pos = lax.broadcasted_iota(jnp.int32, (rows, positions), 1) + kv * positions
    row_l = lax.broadcasted_iota(jnp.int32, (rows, LANES), 0) // GROUP
    lane_l = lax.broadcasted_iota(jnp.int32, (rows, LANES), 1)
    row_g = lax.broadcasted_iota(jnp.int32, (rows, kv_heads), 0) // GROUP
    lane_g = lax.broadcasted_iota(jnp.int32, (rows, kv_heads), 1)

    def attend(b):
        q = q_rows[pl.ds(pl.multiple_of(b * rows, rows), rows), :]
        spread = jnp.concatenate(
            [jnp.where(row_l == g, q, 0.0).astype(BF16) for g in range(heads)], axis=1
        )
        slab = cache[b]
        scores = lax.dot_general(
            spread, slab, (((1,), (1,)), ((), ())), preferred_element_type=F32
        )
        gate_rows = gates[b]
        gate = jnp.broadcast_to(gate_rows[0:1], (rows, positions))
        for g in range(1, heads):
            gate = jnp.where(row_p == g, gate_rows[g : g + 1], gate)
        fresh = jnp.sum(
            jnp.where(lane_g == row_g + tp * heads, gate_now[pl.ds(b, 1), :kv_heads], 0.0),
            axis=1,
            keepdims=True,
        )
        scores = scores + gate + fresh
        live = pos < lengths[b]
        scores = jnp.where(live, scores, EMPTY_SCORE)
        top = jnp.max(scores, axis=1, keepdims=True)
        weights = jnp.where(live, jnp.exp(scores - top), 0.0)
        total = jnp.sum(weights, axis=1, keepdims=True)
        mixed = jnp.dot(weights.astype(BF16), slab, preferred_element_type=F32)
        own = mixed[:, :LANES]
        for g in range(1, heads):
            own = jnp.where(row_l == g, mixed[:, g * LANES : (g + 1) * LANES], own)
        own = jnp.where(lane_l < DH // 2, top, jnp.where(lane_l < DH, total, own))
        return own

    sa, ra = kv_send.at[2], kv_recv.at[2]

    def att_go(i, c):
        peer = partner(i, kv, k_size)
        for e in range(per):
            att_part[peer, e] = attend(peer * per + e)

        @pl.when(i < k_size - 1)
        def _():
            push("kv", peer, kv, att_part.at[peer], att_in, sa, ra).start()

        return c

    lax.fori_loop(0, k_size, att_go, 0)
    att_in[kv] = att_part[kv]
    local[7].wait()
    local[8].wait()
    gain_block = jnp.broadcast_to(wide_gain, (seqs, width)).astype(BF16)
    first_row = lax.broadcasted_iota(jnp.int32, (8, f_chunk), 0) == 0
    sc, rc = kv_send.at[8], kv_recv.at[8]

    def gain_go(i, c):
        peer = partner(i, kv, k_size)
        at = pl.ds(pl.multiple_of(peer * f_chunk, LANES), f_chunk)
        through_gate = jnp.dot(gain_block, wg[:, at], preferred_element_type=F32)
        through_up = jnp.dot(gain_block, wu[:, at], preferred_element_type=F32)
        g_part[peer] = jnp.where(first_row, through_gate[:8], through_up[:8])

        @pl.when(i < k_size - 1)
        def _():
            push("kv", peer, kv, g_part.at[peer], g_in, sc, rc).start()

        return c

    lax.fori_loop(0, k_size, gain_go, 0)
    g_in[kv] = g_part[kv]

    def att_come(i, c):
        arrival("kv", partner(i, kv, k_size), att_part.at[0], att_in, sa, ra).wait_recv()
        return c

    lax.fori_loop(0, k_size - 1, att_come, 0)
    for e in range(per):
        at = pl.ds(pl.multiple_of((kv * per + e) * rows, rows), rows)
        q, pair = q_rows[at, :], kv_rows[at, :]
        own_score = jnp.sum(jnp.where(lane_l < DH, q * pair, 0.0), axis=1, keepdims=True)
        parts = [att_in[k, e] for k in range(k_size)]
        tops = [part[:, 0:1] for part in parts]
        high = own_score
        for top in tops:
            high = jnp.maximum(high, top)
        own_weight = jnp.exp(own_score - high)
        numer = own_weight.astype(BF16).astype(F32) * pair
        denom = own_weight
        for top, part in zip(tops, parts):
            scale = jnp.exp(top - high)
            numer = numer + part * scale
            denom = denom + part[:, DH // 2 : DH // 2 + 1] * scale
        done = numer / denom
        if e % 2 == 0:
            left = pltpu.roll(done, DH, 1)
        else:
            both = jnp.where(lane_l < DH, left, done).astype(BF16)
            att_own[e // 2 * rows : (e // 2 + 1) * rows, :] = both
    kv_all(3, att_own, att_all)
    for k in range(k_size):
        for e in range(per):
            pair = att_all[k, e // 2 * rows : (e // 2 + 1) * rows, :].astype(F32)
            pair = pltpu.roll(pair, DH, 1) if e % 2 == 0 else pair
            q_rows[(k * per + e) * rows : (k * per + e + 1) * rows, :] = pair
    pieces = []
    for h in range(0, rows, 2):
        even = pltpu.roll(q_rows[pl.ds(h, seqs, stride=rows), :], DH, 1)
        odd = q_rows[pl.ds(h + 1, seqs, stride=rows), :]
        pieces.append(jnp.where(lane < DH, even, odd).astype(BF16))
    attended = jnp.concatenate(pieces, axis=1)
    local[6].wait()
    x_own[...] = jnp.dot(attended, wo[...], preferred_element_type=F32)

    def normed(z, phase, stat_own, stat_in):
        row_sum = jnp.sum(z, axis=1, keepdims=True)
        row_square = jnp.sum(z * z, axis=1, keepdims=True)
        stat_own[...] = jnp.where(lane == 0, row_sum, row_square)
        kv_all(phase, stat_own, stat_in)
        stats = stat_in[0]
        for k in range(1, k_size):
            stats = stats + stat_in[k]
        count = k_size * width
        centre = stats[:, 0:1] / count
        spread = stats[:, 1:2] / count - centre * centre
        return (z - centre) * lax.rsqrt(spread + EPSILON)

    tp_all(1, x_own, x_in)
    z = wide[...]
    for t in range(t_size):
        z = z + x_in[t]
    block_mean = jnp.sum(z, axis=1, keepdims=True) / width
    offset = z - block_mean
    s1_own[...] = jnp.where(lane == 0, block_mean, jnp.sum(offset * offset, axis=1, keepdims=True))
    ss, rs = kv_send.at[4], kv_recv.at[4]

    def stat_go(i, c):
        push("kv", partner(i, kv, k_size), kv, s1_own, s1_in, ss, rs).start()
        return c

    lax.fori_loop(0, k_size - 1, stat_go, 0)
    s1_in[kv] = s1_own[...]
    lifted = (offset * wide_gain).astype(BF16)
    sg, rg = kv_send.at[5], kv_recv.at[5]

    def gu_go(i, c):
        peer = partner(i, kv, k_size)
        at = pl.ds(pl.multiple_of(peer * f_chunk, LANES), f_chunk)
        gu_part[peer, 0] = jnp.dot(lifted, wg[:, at], preferred_element_type=F32).astype(BF16)
        gu_part[peer, 1] = jnp.dot(lifted, wu[:, at], preferred_element_type=F32).astype(BF16)

        @pl.when(i < k_size - 1)
        def _():
            push("kv", peer, kv, gu_part.at[peer], gu_in, sg, rg).start()

        return c

    lax.fori_loop(0, k_size, gu_go, 0)
    gu_in[kv] = gu_part[kv]

    def gu_come(i, c):
        arrival("kv", partner(i, kv, k_size), gu_part.at[0], gu_in, sg, rg).wait_recv()
        return c

    def stat_come(i, c):
        peer = partner(i, kv, k_size)
        arrival("kv", peer, s1_own, s1_in, ss, rs).wait_recv()
        arrival("kv", peer, g_part.at[0], g_in, sc, rc).wait_recv()
        return c

    lax.fori_loop(0, k_size - 1, stat_come, 0)
    means = [s1_in[k][:, 0:1] for k in range(k_size)]
    centre = means[0]
    for k in range(1, k_size):
        centre = centre + means[k]
    centre = centre / k_size
    shifts = [mean - centre for mean in means]
    square = jnp.zeros((seqs, 1), F32)
    for k in range(k_size):
        square = square + s1_in[k][:, 1:2] + width * shifts[k] * shifts[k]
    inverse = lax.rsqrt(square / (k_size * width) + EPSILON)
    mid = ((z - centre) * inverse * wide_gain).astype(BF16)
    gate = jnp.zeros((seqs, f_chunk), F32)
    up = jnp.zeros((seqs, f_chunk), F32)
    for k in range(k_size):
        through = g_in[k]
        gate = gate + shifts[k] * through[0:1]
        up = up + shifts[k] * through[1:2]
    lax.fori_loop(0, k_size - 1, gu_come, 0)
    for k in range(k_size):
        gate = gate + gu_in[k, 0].astype(F32)
        up = up + gu_in[k, 1].astype(F32)
    gate = gate * inverse
    up = up * inverse
    hid_own[...] = (gate / (1.0 + jnp.exp(-gate)) * up).astype(BF16)
    local[9].wait()
    sh, rh = kv_send.at[6], kv_recv.at[6]

    def hid_go(i, c):
        push("kv", partner(i, kv, k_size), kv, hid_own, hid_all, sh, rh).start()
        return c

    lax.fori_loop(0, k_size - 1, hid_go, 0)
    hid_all[kv] = hid_own[...]

    def down(i, acc):
        peer = lax.rem(kv + i, k_size)

        @pl.when(i > 0)
        def _():
            arrival("kv", peer, hid_own, hid_all, sh, rh).wait_recv()

        at = pl.ds(pl.multiple_of(peer * f_chunk, LANES), f_chunk)
        return acc + jnp.dot(hid_all[peer], wd[at, :], preferred_element_type=F32)

    y_own[...] = lax.fori_loop(0, k_size, down, jnp.zeros((seqs, width), F32))
    tp_all(2, y_own, y_in)
    z = mid.astype(F32)
    for t in range(t_size):
        z = z + y_in[t]
    wide[...] = normed(z, 7, s2_own, s2_in)
    mine = wide[:, pl.ds(pl.multiple_of(tp * LANES, LANES), LANES)]
    out[...] = (mine * gain_two[...]).astype(BF16)

    for phase, own, landing in ((0, tok_own, tok_all), (1, x_own, x_in), (2, y_own, y_in)):
        for i in range(1, t_size):
            peer = lax.rem(tp + i, t_size)
            arrival("tp", peer, own, landing, tp_send.at[phase], tp_recv.at[phase]).wait_send()

    def finish(i, c):
        peer = partner(i, kv, k_size)

        @pl.when(peer < n_chunks)
        def _():
            arrival("kv", peer, qkv_part.at[peer], qkv_in, s, r).wait_send()

        @pl.when(kv < n_chunks - 1)
        def _():
            arrival("kv", peer, qkv_own, qkv_all, s2, r2).wait_send()

        @pl.when(kv == n_chunks - 1)
        def _():
            arrival("kv", peer, f_own, f_all, s2, r2).wait_send()

        for phase, own, landing in (
            (2, att_part.at[peer], att_in),
            (3, att_own, att_all),
            (4, s1_own, s1_in),
            (5, gu_part.at[peer], gu_in),
            (6, hid_own, hid_all),
            (7, s2_own, s2_in),
            (8, g_part.at[peer], g_in),
        ):
            arrival("kv", peer, own, landing, kv_send.at[phase], kv_recv.at[phase]).wait_send()
        return c

    lax.fori_loop(0, k_size - 1, finish, 0)


def fused(
    tokens,
    live_lengths,
    kv_cache,
    gate_sums,
    w_query,
    w_key,
    w_value,
    w_forget,
    forget_bias,
    w_out,
    first_gain,
    w_gate,
    w_up,
    w_down,
    second_gain,
):
    k_size, t_size = lax.axis_size("kv"), lax.axis_size("tp")
    seqs = tokens.shape[0]
    positions = kv_cache.shape[1]
    heads = kv_cache.shape[2] // (2 * DH)
    rows = heads * GROUP
    row_n, q_cols = w_query.shape
    kk = w_key.shape[1]
    width = w_out.shape[1]
    ff = w_gate.shape[1]
    chunk = kk
    n_chunks = q_cols // chunk + 3
    f_chunk = -(-ff // (k_size * LANES)) * LANES
    padded = f_chunk * k_size
    per = seqs // k_size
    dims = (seqs, k_size, t_size, heads, chunk, n_chunks, f_chunk, positions)
    vmem = pl.BlockSpec(memory_space=pltpu.VMEM)
    smem = pl.BlockSpec(memory_space=pltpu.SMEM)
    hbm = pl.BlockSpec(memory_space=pl.ANY)
    V = pltpu.VMEM
    scratch = [
        V((row_n, q_cols + 2 * kk), BF16),
        V((w_forget.shape[1], row_n), BF16),
        V(kv_cache.shape, BF16),
        V(gate_sums.shape, F32),
        V(w_out.shape, BF16),
        V((row_n, padded), BF16),
        V((row_n, padded), BF16),
        V((padded, width), BF16),
        V((seqs + 8, LANES), F32),
        V((t_size, seqs + 8, LANES), F32),
        V((n_chunks, seqs, chunk), F32),
        V((k_size, seqs, chunk), F32),
        V((seqs, chunk), BF16),
        V((k_size, seqs, chunk), BF16),
        V((seqs, LANES), F32),
        V((k_size, seqs, LANES), F32),
        V((seqs * rows, LANES), F32),
        V((seqs * rows, LANES), F32),
        V((seqs, LANES), F32),
        V((k_size, per, rows, LANES), F32),
        V((k_size, per, rows, LANES), F32),
        V((per // 2 * rows, LANES), BF16),
        V((k_size, per // 2 * rows, LANES), BF16),
        V((seqs, width), F32),
        V((t_size, seqs, width), F32),
        V((seqs, width), F32),
        V((t_size, seqs, width), F32),
        V((seqs, LANES), F32),
        V((k_size, seqs, LANES), F32),
        V((seqs, LANES), F32),
        V((k_size, seqs, LANES), F32),
        V((k_size, 2, seqs, f_chunk), BF16),
        V((k_size, 2, seqs, f_chunk), BF16),
        V((k_size, 8, f_chunk), F32),
        V((k_size, 8, f_chunk), F32),
        V((seqs, f_chunk), BF16),
        V((k_size, seqs, f_chunk), BF16),
        V((seqs, width), F32),
        pltpu.SemaphoreType.DMA((10,)),
        pltpu.SemaphoreType.DMA((3, t_size)),
        pltpu.SemaphoreType.DMA((3, t_size)),
        pltpu.SemaphoreType.DMA((9, k_size)),
        pltpu.SemaphoreType.DMA((9, k_size)),
    ]
    return pl.pallas_call(
        functools.partial(fused_kernel, dims),
        out_shape=jax.ShapeDtypeStruct(tokens.shape, BF16),
        in_specs=[vmem, smem, hbm, hbm, hbm, hbm, hbm, hbm, vmem, hbm, vmem, hbm, hbm, hbm, vmem],
        out_specs=vmem,
        scratch_shapes=scratch,
        compiler_params=pltpu.CompilerParams(
            collective_id=0, has_side_effects=True, vmem_limit_bytes=60 * 1024 * 1024
        ),
    )(
        tokens,
        live_lengths,
        kv_cache,
        gate_sums,
        w_query,
        w_key,
        w_value,
        w_forget.T,
        forget_bias.reshape(1, -1),
        w_out,
        first_gain.reshape(1, -1),
        w_gate,
        w_up,
        w_down,
        second_gain.reshape(1, -1),
    )


def fits(tokens, kv_cache, w_query, w_key, w_gate):
    k_size = lax.axis_size("kv")
    heads = kv_cache.shape[2] // (2 * DH)
    return (
        tokens.shape[1] == LANES
        and tokens.shape[0] % 16 == 0
        and tokens.shape[0] % (2 * k_size) == 0
        and k_size % 2 == 0
        and heads % 2 == 0
        and w_key.shape[1] % LANES == 0
        and w_query.shape[1] % w_key.shape[1] == 0
        and w_query.shape[1] // w_key.shape[1] + 3 <= k_size
        and w_gate.shape[1] % LANES == 0
    )


def choose(*args):
    if fits(args[0], args[2], args[4], args[5], args[11]):
        return fused(*args)
    return on_device(*args)


def solution(mesh):
    in_specs = (
        P(None, ("kv", "tp")),
        P(),
        P(None, "kv", "tp"),
        P(None, "tp", "kv"),
        P("kv", "tp"),
        P("kv", "tp"),
        P("kv", "tp"),
        P(),
        P(),
        P("tp", "kv"),
        P(("kv", "tp")),
        P("kv", "tp"),
        P("kv", "tp"),
        P("tp", "kv"),
        P(("kv", "tp")),
    )
    out_specs = P(None, ("kv", "tp"))
    return jax.shard_map(
        choose, mesh=mesh, in_specs=in_specs, out_specs=out_specs, check_vma=False
    )
```

```python
import functools

import jax
import jax.numpy as jnp
from jax import lax
from jax.experimental import pallas as pl
from jax.experimental.pallas import tpu as pltpu
from jax.sharding import PartitionSpec as P

D = 4096
DH = 64
GROUP = 4


EPSILON = 1e-05
EMPTY_SCORE = -1e30


def combined_all(shard, axis, combine):
    everything = jax.tree.map(lambda part: lax.all_gather(part, axis), shard)
    initial = jax.tree.map(lambda part: part[0], everything)

    def lap(k, so_far):
        return combine(so_far, jax.tree.map(lambda part: part[k], everything))

    return lax.fori_loop(1, lax.axis_size(axis), lap, initial)


def combine_parts(earlier, later):
    earlier_top, earlier_total, earlier_sum = earlier
    later_top, later_total, later_sum = later
    joint_top = jnp.maximum(earlier_top, later_top)
    earlier_scale = jnp.exp(earlier_top - joint_top)
    later_scale = jnp.exp(later_top - joint_top)
    joint_total = earlier_total * earlier_scale + later_total * later_scale
    joint_sum = earlier_sum * earlier_scale[..., None] + later_sum * later_scale[..., None]
    return (joint_top, joint_total, joint_sum)


def normalize_block(mixture, norm_gain):
    row_sum, row_square = lax.psum(
        (jnp.sum(mixture, axis=1), jnp.sum(mixture * mixture, axis=1)), "kv"
    )
    centre = row_sum / D
    spread = row_square / D - centre * centre
    scaled = (mixture - centre[:, None]) * lax.rsqrt(spread[:, None] + EPSILON) * norm_gain
    return scaled.astype(jnp.bfloat16)


def on_device(
    tokens,
    live_lengths,
    kv_cache,
    gate_sums,
    w_query,
    w_key,
    w_value,
    w_forget,
    forget_bias,
    w_out,
    first_gain,
    w_gate,
    w_up,
    w_down,
    second_gain,
):
    sequences = tokens.shape[0]
    own_cols = tokens.shape[1]
    gains_pair = jnp.stack([first_gain, second_gain], axis=0)
    wide_rows, wide_gains = (
        lax.all_gather(tokens.astype(jnp.float32), "tp", axis=1, tiled=True),
        lax.all_gather(gains_pair, "tp", axis=1, tiled=True),
    )
    block_rows = wide_rows.astype(jnp.bfloat16)
    row_count = block_rows.shape[1]
    row_start = lax.axis_index("kv") * row_count
    local_heads = kv_cache.shape[2] // (2 * DH)
    head_start = lax.axis_index("tp") * local_heads
    forget_rows = lax.dynamic_slice(w_forget, (row_start, head_start), (row_count, local_heads))
    query_part = jnp.dot(block_rows, w_query, preferred_element_type=jnp.float32)
    key_part = jnp.dot(block_rows, w_key, preferred_element_type=jnp.float32)
    value_part = jnp.dot(block_rows, w_value, preferred_element_type=jnp.float32)
    forget_part = jnp.dot(block_rows, forget_rows, preferred_element_type=jnp.float32)
    query_sum, key_sum, value_sum, forget_sum = lax.psum(
        (query_part, key_part, value_part, forget_part), "kv"
    )
    queries = query_sum.astype(jnp.bfloat16).reshape(sequences, local_heads, GROUP, DH)
    new_keys = key_sum.astype(jnp.bfloat16).reshape(sequences, local_heads, DH)
    new_values = value_sum.astype(jnp.bfloat16).reshape(sequences, local_heads, DH)
    bias_rows = lax.dynamic_slice_in_dim(forget_bias, head_start, local_heads)
    new_gate = jax.nn.log_sigmoid(forget_sum + bias_rows)
    positions = kv_cache.shape[1]
    cached = kv_cache.reshape(sequences, positions, local_heads, 2, DH)
    score_scale = DH ** (-0.5)
    scores = (
        jnp.einsum(
            "bgjd,bpgd->bgjp", queries, cached[:, :, :, 0], preferred_element_type=jnp.float32
        )
        * score_scale
    )
    scores = scores + gate_sums[:, :, None, :] + new_gate[:, :, None, None]
    position_selector = lax.axis_index("kv") * positions + jnp.arange(positions, dtype=jnp.int32)
    live_mask = (position_selector[None, :] < live_lengths[:, None])[:, None, None, :]
    local_top = jnp.max(jnp.where(live_mask, scores, EMPTY_SCORE), axis=-1)
    weights = jnp.where(live_mask, jnp.exp(scores - local_top[..., None]), 0.0)
    local_total = jnp.sum(weights, axis=-1)
    local_sum = jnp.einsum(
        "bgjp,bpgd->bgjd",
        weights.astype(jnp.bfloat16),
        cached[:, :, :, 1],
        preferred_element_type=jnp.float32,
    )
    row_top, weight_total, summed = combined_all(
        (local_top, local_total, local_sum), "kv", combine_parts
    )
    own_score = (
        jnp.einsum("bgjd,bgd->bgj", queries, new_keys, preferred_element_type=jnp.float32)
        * score_scale
    )
    final_top = jnp.maximum(row_top, own_score)
    carry_scale = jnp.exp(row_top - final_top)
    own_weight = jnp.exp(own_score - final_top)
    own_rounded = lax.optimization_barrier(own_weight.astype(jnp.bfloat16)).astype(jnp.float32)
    numerator = summed * carry_scale[..., None] + own_rounded[..., None] * new_values[
        :, :, None, :
    ].astype(jnp.float32)
    attended = (numerator / (weight_total * carry_scale + own_weight)[..., None]).astype(
        jnp.bfloat16
    )
    attended = attended.reshape(sequences, local_heads * GROUP * DH)
    attn_part = jnp.dot(attended, w_out, preferred_element_type=jnp.float32)
    attn_block = lax.psum(attn_part, "tp")
    mid_rows = normalize_block(wide_rows + attn_block, wide_gains[0])
    gate_part = jnp.dot(mid_rows, w_gate, preferred_element_type=jnp.float32)
    up_part = jnp.dot(mid_rows, w_up, preferred_element_type=jnp.float32)
    gate_full, up_full = (
        lax.psum(gate_part.astype(jnp.bfloat16), "kv").astype(jnp.float32),
        lax.psum(up_part.astype(jnp.bfloat16), "kv").astype(jnp.float32),
    )
    hidden = (jax.nn.silu(gate_full) * up_full).astype(jnp.bfloat16)
    ffn_part = jnp.dot(hidden, w_down, preferred_element_type=jnp.float32)
    ffn_block = lax.psum(ffn_part, "tp")
    out_block = normalize_block(mid_rows.astype(jnp.float32) + ffn_block, wide_gains[1])
    return lax.dynamic_slice_in_dim(out_block, lax.axis_index("tp") * own_cols, own_cols, 1)


MESH = pl.DeviceIdType.MESH
F32 = jnp.float32
BF16 = jnp.bfloat16
LANES = 128


def push(axis, peer, me, source, landing, sends, recvs):
    return pltpu.make_async_remote_copy(
        src_ref=source,
        dst_ref=landing.at[me],
        send_sem=sends.at[peer],
        recv_sem=recvs.at[me],
        device_id={axis: peer},
        device_id_type=MESH,
    )


def partner(m, me, size):
    return lax.rem(me + 1 + m, size)


def arrival(axis, peer, source, landing, sends, recvs):
    return pltpu.make_async_remote_copy(
        src_ref=source,
        dst_ref=landing.at[peer],
        send_sem=sends.at[peer],
        recv_sem=recvs.at[peer],
        device_id={axis: peer},
        device_id_type=MESH,
    )


def head_rows(block, odd, lane):
    moved = pltpu.roll(block, DH, 1) if odd else block
    return jnp.where(lane < DH, moved, 0.0)


def fused_kernel(
    dims,
    tokens,
    lengths,
    cache_hbm,
    gates_hbm,
    wq_hbm,
    wk_hbm,
    wv_hbm,
    wf_hbm,
    bias,
    wo_hbm,
    gain_one,
    wg_hbm,
    wu_hbm,
    wd_hbm,
    gain_two,
    out,
    wqkv,
    wf,
    cache,
    gates,
    wo,
    wg,
    wu,
    wd,
    tok_own,
    tok_all,
    qkv_part,
    qkv_in,
    qkv_own,
    qkv_all,
    f_own,
    f_all,
    q_rows,
    kv_rows,
    gate_now,
    att_part,
    att_in,
    att_own,
    att_all,
    x_own,
    x_in,
    y_own,
    y_in,
    s1_own,
    s1_in,
    s2_own,
    s2_in,
    gu_part,
    gu_in,
    g_part,
    g_in,
    hid_own,
    hid_all,
    wide,
    sems,
    tp_send,
    tp_recv,
    kv_send,
    kv_recv,
):
    seqs, k_size, t_size, heads, chunk, n_chunks, f_chunk, positions = dims
    kv = lax.axis_index("kv")
    tp = lax.axis_index("tp")
    rows_n = wq_hbm.shape[0]
    q_cols = wq_hbm.shape[1]
    kk = wk_hbm.shape[1]
    ff = wg_hbm.shape[1]
    width = wo_hbm.shape[1]
    per = seqs // k_size
    rows = heads * GROUP
    local = [
        pltpu.make_async_copy(wq_hbm, wqkv.at[:, :q_cols], sems.at[0]),
        pltpu.make_async_copy(wk_hbm, wqkv.at[:, q_cols : q_cols + kk], sems.at[1]),
        pltpu.make_async_copy(wv_hbm, wqkv.at[:, q_cols + kk :], sems.at[2]),
        pltpu.make_async_copy(
            wf_hbm.at[:, pl.ds(pl.multiple_of(kv * rows_n, rows_n), rows_n)], wf, sems.at[3]
        ),
        pltpu.make_async_copy(cache_hbm, cache, sems.at[4]),
        pltpu.make_async_copy(gates_hbm, gates, sems.at[5]),
        pltpu.make_async_copy(wo_hbm, wo, sems.at[6]),
        pltpu.make_async_copy(wg_hbm, wg.at[:, :ff], sems.at[7]),
        pltpu.make_async_copy(wu_hbm, wu.at[:, :ff], sems.at[8]),
        pltpu.make_async_copy(wd_hbm, wd.at[:ff, :], sems.at[9]),
    ]
    barrier = pltpu.get_barrier_semaphore()
    for i in range(k_size - 1):
        pl.semaphore_signal(
            barrier, inc=1, device_id={"kv": partner(i, kv, k_size)}, device_id_type=MESH
        )
    for i in range(1, t_size):
        pl.semaphore_signal(
            barrier, inc=1, device_id={"tp": lax.rem(tp + i, t_size)}, device_id_type=MESH
        )
    for copy in local:
        copy.start()
    padded = wg.shape[1]
    if padded > ff:
        wg[:, ff:] = jnp.zeros((rows_n, padded - ff), BF16)
        wu[:, ff:] = jnp.zeros((rows_n, padded - ff), BF16)
        wd[ff:, :] = jnp.zeros((padded - ff, width), BF16)
    tok_own[:seqs, :] = tokens[...].astype(F32)
    tok_own[seqs:, :] = jnp.broadcast_to(gain_one[...], (8, LANES))
    pl.semaphore_wait(barrier, k_size - 1 + t_size - 1)

    def tp_all(phase, own, landing):
        s, r = tp_send.at[phase], tp_recv.at[phase]
        for i in range(1, t_size):
            push("tp", lax.rem(tp + i, t_size), tp, own, landing, s, r).start()
        landing[tp] = own[...]
        for i in range(1, t_size):
            arrival("tp", lax.rem(tp + i, t_size), own, landing, s, r).wait_recv()

    def kv_all(phase, own, landing):
        s, r = kv_send.at[phase], kv_recv.at[phase]

        def go(i, c):
            push("kv", partner(i, kv, k_size), kv, own, landing, s, r).start()
            return c

        def come(i, c):
            arrival("kv", partner(i, kv, k_size), own, landing, s, r).wait_recv()
            return c

        lax.fori_loop(0, k_size - 1, go, 0)
        landing[kv] = own[...]
        lax.fori_loop(0, k_size - 1, come, 0)

    tp_all(0, tok_own, tok_all)
    wide_rows = jnp.concatenate([tok_all[t, :seqs, :] for t in range(t_size)], axis=1)
    wide_gain = jnp.concatenate([tok_all[t, seqs : seqs + 1, :] for t in range(t_size)], axis=1)
    wide[...] = wide_rows
    block = wide_rows.astype(BF16)
    for n in range(4):
        local[n].wait()
    for c in range(n_chunks - 1):
        qkv_part[c] = jnp.dot(
            block, wqkv[:, c * chunk : (c + 1) * chunk], preferred_element_type=F32
        )
    kv_heads = wf.shape[0]
    qkv_part[n_chunks - 1] = jnp.zeros((seqs, chunk), F32)
    qkv_part[n_chunks - 1, :, :kv_heads] = lax.dot_general(
        block, wf[...], (((1,), (1,)), ((), ())), preferred_element_type=F32
    )
    s, r = kv_send.at[0], kv_recv.at[0]
    s2, r2 = kv_send.at[1], kv_recv.at[1]

    def qkv_go(i, c):
        peer = partner(i, kv, k_size)

        @pl.when(peer < n_chunks)
        def _():
            push("kv", peer, kv, qkv_part.at[peer], qkv_in, s, r).start()

        return c

    lax.fori_loop(0, k_size - 1, qkv_go, 0)

    @pl.when(kv < n_chunks)
    def _():
        qkv_in[kv] = qkv_part[kv]

        def come(i, c):
            peer = partner(i, kv, k_size)
            arrival("kv", peer, qkv_part.at[0], qkv_in, s, r).wait_recv()
            return c

        lax.fori_loop(0, k_size - 1, come, 0)
        total = qkv_in[0]
        for k in range(1, k_size):
            total = total + qkv_in[k]
        scale = jnp.where(kv < q_cols // chunk, DH**-0.5, 1.0).astype(F32)
        qkv_own[...] = (total.astype(BF16).astype(F32) * scale).astype(BF16)
        f_own[...] = total[:, :LANES]

        @pl.when(kv < n_chunks - 1)
        def _():
            def go(i, c):
                push("kv", partner(i, kv, k_size), kv, qkv_own, qkv_all, s2, r2).start()
                return c

            lax.fori_loop(0, k_size - 1, go, 0)
            qkv_all[kv] = qkv_own[...]

        @pl.when(kv == n_chunks - 1)
        def _():
            def go(i, c):
                push("kv", partner(i, kv, k_size), kv, f_own, f_all, s2, r2).start()
                return c

            lax.fori_loop(0, k_size - 1, go, 0)
            f_all[kv] = f_own[...]

    def qkv_come(i, c):
        peer = partner(i, kv, k_size)

        @pl.when(peer < n_chunks - 1)
        def _():
            arrival("kv", peer, qkv_own, qkv_all, s2, r2).wait_recv()

        @pl.when(peer == n_chunks - 1)
        def _():
            arrival("kv", peer, f_own, f_all, s2, r2).wait_recv()

        return c

    local[7].wait()
    local[8].wait()
    gain_block = jnp.broadcast_to(wide_gain, (seqs, width)).astype(BF16)
    first_row = lax.broadcasted_iota(jnp.int32, (8, f_chunk), 0) == 0
    sc, rc = kv_send.at[8], kv_recv.at[8]

    def gain_go(i, c):
        peer = partner(i, kv, k_size)
        at = pl.ds(pl.multiple_of(peer * f_chunk, LANES), f_chunk)
        through_gate = jnp.dot(gain_block, wg[:, at], preferred_element_type=F32)
        through_up = jnp.dot(gain_block, wu[:, at], preferred_element_type=F32)
        g_part[peer] = jnp.where(first_row, through_gate[:8], through_up[:8])

        @pl.when(i < k_size - 1)
        def _():
            push("kv", peer, kv, g_part.at[peer], g_in, sc, rc).start()

        return c

    lax.fori_loop(0, k_size, gain_go, 0)
    g_in[kv] = g_part[kv]
    lax.fori_loop(0, k_size - 1, qkv_come, 0)
    lane = lax.broadcasted_iota(jnp.int32, (seqs, LANES), 1)

    def unit(start):
        return qkv_all[start // chunk, :, start % chunk : start % chunk + LANES].astype(F32)

    for h in range(rows):
        start = h * DH
        base = start // LANES * LANES
        q_rows[pl.ds(h, seqs, stride=rows), :] = head_rows(unit(base), start % LANES != 0, lane)
    for g in range(heads):
        base = g * DH // LANES * LANES
        odd = g % 2 == 1
        keys = unit(q_cols + base)
        values = unit(q_cols + kk + base)
        keys = pltpu.roll(keys, DH, 1) if odd else keys
        values = values if odd else pltpu.roll(values, DH, 1)
        pair = jnp.where(lane < DH, keys, values)
        for j in range(GROUP):
            kv_rows[pl.ds(g * GROUP + j, seqs, stride=rows), :] = pair
    logits = f_all[n_chunks - 1, :, :kv_heads] + bias[...]
    gate_now[:, :kv_heads] = jnp.minimum(logits, 0.0) - jnp.log(1.0 + jnp.exp(-jnp.abs(logits)))
    local[4].wait()
    local[5].wait()
    row_p = lax.broadcasted_iota(jnp.int32, (rows, positions), 0) // GROUP
    pos = lax.broadcasted_iota(jnp.int32, (rows, positions), 1) + kv * positions
    row_l = lax.broadcasted_iota(jnp.int32, (rows, LANES), 0) // GROUP
    lane_l = lax.broadcasted_iota(jnp.int32, (rows, LANES), 1)
    row_g = lax.broadcasted_iota(jnp.int32, (rows, kv_heads), 0) // GROUP
    lane_g = lax.broadcasted_iota(jnp.int32, (rows, kv_heads), 1)

    def attend(b):
        q = q_rows[pl.ds(pl.multiple_of(b * rows, rows), rows), :]
        spread = jnp.concatenate(
            [jnp.where(row_l == g, q, 0.0).astype(BF16) for g in range(heads)], axis=1
        )
        slab = cache[b]
        scores = lax.dot_general(
            spread, slab, (((1,), (1,)), ((), ())), preferred_element_type=F32
        )
        gate_rows = gates[b]
        gate = jnp.broadcast_to(gate_rows[0:1], (rows, positions))
        for g in range(1, heads):
            gate = jnp.where(row_p == g, gate_rows[g : g + 1], gate)
        fresh = jnp.sum(
            jnp.where(lane_g == row_g + tp * heads, gate_now[pl.ds(b, 1), :kv_heads], 0.0),
            axis=1,
            keepdims=True,
        )
        scores = scores + gate + fresh
        live = pos < lengths[b]
        scores = jnp.where(live, scores, EMPTY_SCORE)
        top = jnp.max(scores, axis=1, keepdims=True)
        weights = jnp.where(live, jnp.exp(scores - top), 0.0)
        total = jnp.sum(weights, axis=1, keepdims=True)
        mixed = jnp.dot(weights.astype(BF16), slab, preferred_element_type=F32)
        own = mixed[:, :LANES]
        for g in range(1, heads):
            own = jnp.where(row_l == g, mixed[:, g * LANES : (g + 1) * LANES], own)
        own = jnp.where(lane_l < DH // 2, top, jnp.where(lane_l < DH, total, own))
        return own

    sa, ra = kv_send.at[2], kv_recv.at[2]

    def att_go(i, c):
        peer = partner(i, kv, k_size)
        for e in range(per):
            att_part[peer, e] = attend(peer * per + e)

        @pl.when(i < k_size - 1)
        def _():
            push("kv", peer, kv, att_part.at[peer], att_in, sa, ra).start()

        return c

    lax.fori_loop(0, k_size, att_go, 0)
    att_in[kv] = att_part[kv]

    def att_come(i, c):
        arrival("kv", partner(i, kv, k_size), att_part.at[0], att_in, sa, ra).wait_recv()
        return c

    lax.fori_loop(0, k_size - 1, att_come, 0)
    for e in range(per):
        at = pl.ds(pl.multiple_of((kv * per + e) * rows, rows), rows)
        q, pair = q_rows[at, :], kv_rows[at, :]
        own_score = jnp.sum(jnp.where(lane_l < DH, q * pair, 0.0), axis=1, keepdims=True)
        parts = [att_in[k, e] for k in range(k_size)]
        tops = [part[:, 0:1] for part in parts]
        high = own_score
        for top in tops:
            high = jnp.maximum(high, top)
        own_weight = jnp.exp(own_score - high)
        numer = own_weight.astype(BF16).astype(F32) * pair
        denom = own_weight
        for top, part in zip(tops, parts):
            scale = jnp.exp(top - high)
            numer = numer + part * scale
            denom = denom + part[:, DH // 2 : DH // 2 + 1] * scale
        done = numer / denom
        if e % 2 == 0:
            left = pltpu.roll(done, DH, 1)
        else:
            both = jnp.where(lane_l < DH, left, done).astype(BF16)
            att_own[e // 2 * rows : (e // 2 + 1) * rows, :] = both
    kv_all(3, att_own, att_all)
    for k in range(k_size):
        for e in range(per):
            pair = att_all[k, e // 2 * rows : (e // 2 + 1) * rows, :].astype(F32)
            pair = pltpu.roll(pair, DH, 1) if e % 2 == 0 else pair
            q_rows[(k * per + e) * rows : (k * per + e + 1) * rows, :] = pair
    pieces = []
    for h in range(0, rows, 2):
        even = pltpu.roll(q_rows[pl.ds(h, seqs, stride=rows), :], DH, 1)
        odd = q_rows[pl.ds(h + 1, seqs, stride=rows), :]
        pieces.append(jnp.where(lane < DH, even, odd).astype(BF16))
    attended = jnp.concatenate(pieces, axis=1)
    local[6].wait()
    x_own[...] = jnp.dot(attended, wo[...], preferred_element_type=F32)

    def normed(z, phase, stat_own, stat_in):
        row_sum = jnp.sum(z, axis=1, keepdims=True)
        row_square = jnp.sum(z * z, axis=1, keepdims=True)
        stat_own[...] = jnp.where(lane == 0, row_sum, row_square)
        kv_all(phase, stat_own, stat_in)
        stats = stat_in[0]
        for k in range(1, k_size):
            stats = stats + stat_in[k]
        count = k_size * width
        centre = stats[:, 0:1] / count
        spread = stats[:, 1:2] / count - centre * centre
        return (z - centre) * lax.rsqrt(spread + EPSILON)

    tp_all(1, x_own, x_in)
    z = wide[...]
    for t in range(t_size):
        z = z + x_in[t]
    block_mean = jnp.sum(z, axis=1, keepdims=True) / width
    offset = z - block_mean
    s1_own[...] = jnp.where(lane == 0, block_mean, jnp.sum(offset * offset, axis=1, keepdims=True))
    ss, rs = kv_send.at[4], kv_recv.at[4]

    def stat_go(i, c):
        push("kv", partner(i, kv, k_size), kv, s1_own, s1_in, ss, rs).start()
        return c

    lax.fori_loop(0, k_size - 1, stat_go, 0)
    s1_in[kv] = s1_own[...]
    lifted = (offset * wide_gain).astype(BF16)
    sg, rg = kv_send.at[5], kv_recv.at[5]

    def gu_go(i, c):
        peer = partner(i, kv, k_size)
        at = pl.ds(pl.multiple_of(peer * f_chunk, LANES), f_chunk)
        gu_part[peer, 0] = jnp.dot(lifted, wg[:, at], preferred_element_type=F32).astype(BF16)
        gu_part[peer, 1] = jnp.dot(lifted, wu[:, at], preferred_element_type=F32).astype(BF16)

        @pl.when(i < k_size - 1)
        def _():
            push("kv", peer, kv, gu_part.at[peer], gu_in, sg, rg).start()

        return c

    lax.fori_loop(0, k_size, gu_go, 0)
    gu_in[kv] = gu_part[kv]

    def gu_come(i, c):
        arrival("kv", partner(i, kv, k_size), gu_part.at[0], gu_in, sg, rg).wait_recv()
        return c

    def stat_come(i, c):
        peer = partner(i, kv, k_size)
        arrival("kv", peer, s1_own, s1_in, ss, rs).wait_recv()
        arrival("kv", peer, g_part.at[0], g_in, sc, rc).wait_recv()
        return c

    lax.fori_loop(0, k_size - 1, stat_come, 0)
    means = [s1_in[k][:, 0:1] for k in range(k_size)]
    centre = means[0]
    for k in range(1, k_size):
        centre = centre + means[k]
    centre = centre / k_size
    shifts = [mean - centre for mean in means]
    square = jnp.zeros((seqs, 1), F32)
    for k in range(k_size):
        square = square + s1_in[k][:, 1:2] + width * shifts[k] * shifts[k]
    inverse = lax.rsqrt(square / (k_size * width) + EPSILON)
    mid = ((z - centre) * inverse * wide_gain).astype(BF16)
    gate = jnp.zeros((seqs, f_chunk), F32)
    up = jnp.zeros((seqs, f_chunk), F32)
    for k in range(k_size):
        through = g_in[k]
        gate = gate + shifts[k] * through[0:1]
        up = up + shifts[k] * through[1:2]
    lax.fori_loop(0, k_size - 1, gu_come, 0)
    for k in range(k_size):
        gate = gate + gu_in[k, 0].astype(F32)
        up = up + gu_in[k, 1].astype(F32)
    gate = gate * inverse
    up = up * inverse
    hid_own[...] = (gate / (1.0 + jnp.exp(-gate)) * up).astype(BF16)
    local[9].wait()
    sh, rh = kv_send.at[6], kv_recv.at[6]

    def hid_go(i, c):
        push("kv", partner(i, kv, k_size), kv, hid_own, hid_all, sh, rh).start()
        return c

    lax.fori_loop(0, k_size - 1, hid_go, 0)
    hid_all[kv] = hid_own[...]

    def down(i, acc):
        peer = lax.rem(kv + i, k_size)

        @pl.when(i > 0)
        def _():
            arrival("kv", peer, hid_own, hid_all, sh, rh).wait_recv()

        at = pl.ds(pl.multiple_of(peer * f_chunk, LANES), f_chunk)
        return acc + jnp.dot(hid_all[peer], wd[at, :], preferred_element_type=F32)

    y_own[...] = lax.fori_loop(0, k_size, down, jnp.zeros((seqs, width), F32))
    tp_all(2, y_own, y_in)
    z = mid.astype(F32)
    for t in range(t_size):
        z = z + y_in[t]
    wide[...] = normed(z, 7, s2_own, s2_in)
    mine = wide[:, pl.ds(pl.multiple_of(tp * LANES, LANES), LANES)]
    out[...] = (mine * gain_two[...]).astype(BF16)

    for phase, own, landing in ((0, tok_own, tok_all), (1, x_own, x_in), (2, y_own, y_in)):
        for i in range(1, t_size):
            peer = lax.rem(tp + i, t_size)
            arrival("tp", peer, own, landing, tp_send.at[phase], tp_recv.at[phase]).wait_send()

    def finish(i, c):
        peer = partner(i, kv, k_size)

        @pl.when(peer < n_chunks)
        def _():
            arrival("kv", peer, qkv_part.at[peer], qkv_in, s, r).wait_send()

        @pl.when(kv < n_chunks - 1)
        def _():
            arrival("kv", peer, qkv_own, qkv_all, s2, r2).wait_send()

        @pl.when(kv == n_chunks - 1)
        def _():
            arrival("kv", peer, f_own, f_all, s2, r2).wait_send()

        for phase, own, landing in (
            (2, att_part.at[peer], att_in),
            (3, att_own, att_all),
            (4, s1_own, s1_in),
            (5, gu_part.at[peer], gu_in),
            (6, hid_own, hid_all),
            (7, s2_own, s2_in),
            (8, g_part.at[peer], g_in),
        ):
            arrival("kv", peer, own, landing, kv_send.at[phase], kv_recv.at[phase]).wait_send()
        return c

    lax.fori_loop(0, k_size - 1, finish, 0)


def fused(
    tokens,
    live_lengths,
    kv_cache,
    gate_sums,
    w_query,
    w_key,
    w_value,
    w_forget,
    forget_bias,
    w_out,
    first_gain,
    w_gate,
    w_up,
    w_down,
    second_gain,
):
    k_size, t_size = lax.axis_size("kv"), lax.axis_size("tp")
    seqs = tokens.shape[0]
    positions = kv_cache.shape[1]
    heads = kv_cache.shape[2] // (2 * DH)
    rows = heads * GROUP
    row_n, q_cols = w_query.shape
    kk = w_key.shape[1]
    width = w_out.shape[1]
    ff = w_gate.shape[1]
    chunk = kk
    n_chunks = q_cols // chunk + 3
    f_chunk = -(-ff // (k_size * LANES)) * LANES
    padded = f_chunk * k_size
    per = seqs // k_size
    dims = (seqs, k_size, t_size, heads, chunk, n_chunks, f_chunk, positions)
    vmem = pl.BlockSpec(memory_space=pltpu.VMEM)
    smem = pl.BlockSpec(memory_space=pltpu.SMEM)
    hbm = pl.BlockSpec(memory_space=pl.ANY)
    V = pltpu.VMEM
    scratch = [
        V((row_n, q_cols + 2 * kk), BF16),
        V((w_forget.shape[1], row_n), BF16),
        V(kv_cache.shape, BF16),
        V(gate_sums.shape, F32),
        V(w_out.shape, BF16),
        V((row_n, padded), BF16),
        V((row_n, padded), BF16),
        V((padded, width), BF16),
        V((seqs + 8, LANES), F32),
        V((t_size, seqs + 8, LANES), F32),
        V((n_chunks, seqs, chunk), F32),
        V((k_size, seqs, chunk), F32),
        V((seqs, chunk), BF16),
        V((k_size, seqs, chunk), BF16),
        V((seqs, LANES), F32),
        V((k_size, seqs, LANES), F32),
        V((seqs * rows, LANES), F32),
        V((seqs * rows, LANES), F32),
        V((seqs, LANES), F32),
        V((k_size, per, rows, LANES), F32),
        V((k_size, per, rows, LANES), F32),
        V((per // 2 * rows, LANES), BF16),
        V((k_size, per // 2 * rows, LANES), BF16),
        V((seqs, width), F32),
        V((t_size, seqs, width), F32),
        V((seqs, width), F32),
        V((t_size, seqs, width), F32),
        V((seqs, LANES), F32),
        V((k_size, seqs, LANES), F32),
        V((seqs, LANES), F32),
        V((k_size, seqs, LANES), F32),
        V((k_size, 2, seqs, f_chunk), BF16),
        V((k_size, 2, seqs, f_chunk), BF16),
        V((k_size, 8, f_chunk), F32),
        V((k_size, 8, f_chunk), F32),
        V((seqs, f_chunk), BF16),
        V((k_size, seqs, f_chunk), BF16),
        V((seqs, width), F32),
        pltpu.SemaphoreType.DMA((10,)),
        pltpu.SemaphoreType.DMA((3, t_size)),
        pltpu.SemaphoreType.DMA((3, t_size)),
        pltpu.SemaphoreType.DMA((9, k_size)),
        pltpu.SemaphoreType.DMA((9, k_size)),
    ]
    return pl.pallas_call(
        functools.partial(fused_kernel, dims),
        out_shape=jax.ShapeDtypeStruct(tokens.shape, BF16),
        in_specs=[vmem, smem, hbm, hbm, hbm, hbm, hbm, hbm, vmem, hbm, vmem, hbm, hbm, hbm, vmem],
        out_specs=vmem,
        scratch_shapes=scratch,
        compiler_params=pltpu.CompilerParams(
            collective_id=0, has_side_effects=True, vmem_limit_bytes=60 * 1024 * 1024
        ),
    )(
        tokens,
        live_lengths,
        kv_cache,
        gate_sums,
        w_query,
        w_key,
        w_value,
        w_forget.T,
        forget_bias.reshape(1, -1),
        w_out,
        first_gain.reshape(1, -1),
        w_gate,
        w_up,
        w_down,
        second_gain.reshape(1, -1),
    )


def fits(tokens, kv_cache, w_query, w_key, w_gate):
    k_size = lax.axis_size("kv")
    heads = kv_cache.shape[2] // (2 * DH)
    return (
        tokens.shape[1] == LANES
        and tokens.shape[0] % 16 == 0
        and tokens.shape[0] % (2 * k_size) == 0
        and k_size % 2 == 0
        and heads % 2 == 0
        and w_key.shape[1] % LANES == 0
        and w_query.shape[1] % w_key.shape[1] == 0
        and w_query.shape[1] // w_key.shape[1] + 3 <= k_size
        and w_gate.shape[1] % LANES == 0
    )


def choose(*args):
    if fits(args[0], args[2], args[4], args[5], args[11]):
        return fused(*args)
    return on_device(*args)


def solution(mesh):
    in_specs = (
        P(None, ("kv", "tp")),
        P(),
        P(None, "kv", "tp"),
        P(None, "tp", "kv"),
        P("kv", "tp"),
        P("kv", "tp"),
        P("kv", "tp"),
        P(),
        P(),
        P("tp", "kv"),
        P(("kv", "tp")),
        P("kv", "tp"),
        P("kv", "tp"),
        P("tp", "kv"),
        P(("kv", "tp")),
    )
    out_specs = P(None, ("kv", "tp"))
    return jax.shard_map(
        choose, mesh=mesh, in_specs=in_specs, out_specs=out_specs, check_vma=False
    )
```
